256 devices in a mesh: grp: 2 (over y), kv: 16 (over z), tp: 8 (over x, core).
Axes of the slice: x: 4, y: 2, z: 16, core: 2. Of those that a mesh axis runs over, the one named last changes fastest.
The devices are a block of a 4x16x16 slice.
Arguments:
- tokens: bfloat16 [2048, 8, 4096], P('kv', 'grp'), parts along dimension 1, may hold values from -72 to 72
- lengths: int32 [8], P('grp'), parts along dimension 0, may hold values from 1 to 2048, 3072 in all
- chosen: int32 [8, 32, 32, 8], P('grp', 'tp', 'kv'), parts along dimension 0, may hold values from -1 to 31, as said below
- w_query: bfloat16 [4096, 2048], P(None, 'tp'), may hold values from -0.09375 to 0.09375
- w_key: bfloat16 [4096, 2048], P(None, 'tp'), may hold values from -0.09375 to 0.09375
- w_value: bfloat16 [4096, 2048], P(None, 'tp'), may hold values from -0.09375 to 0.09375
- w_gate: bfloat16 [4096, 2, 32], P(None, None, 'tp'), may hold values from -0.09375 to 0.09375
- pool_weights: float32 [2, 32, 64], replicated, may hold values from -1 to 1
- w_out: bfloat16 [2048, 4096], P(None, 'tp'), may hold values from -0.5 to 0.5
Outputs:
- mixed: bfloat16 [2048, 8, 4096], P(('kv', 'tp'), 'grp'), parts along dimension 1
The draws below stay inside these ranges and needn't reach their ends.
There are 2 independent parts, one for each index of `grp`. The reference program is written for one: setup_inputs(seed, part) draws one part's arguments, and reference() takes and returns one part's arrays. A program takes and returns all parts, laid end to end along the dimension named above; an argument that names none is the same for every part. Nothing has to cross between parts.
Inputs may be any that keep to these rules, and one draw needn't show every extreme that they name: `chosen`: for query block b the live slots hold min(8, b+1) distinct blocks, all <= b, among them b, b-1 (when b >= 1) and 0; the other slots are -1.
All inputs are finite; a program needn't handle non-finite values.
Results may differ from the reference program's by a relative error of at most 0.014.
Values may be sent and summed in bfloat16 or wider, within the bound.
A program may use at most 128 MiB of HBM per device.

```python
import math
import jax
import jax.numpy as jnp
import numpy as np
from jax import lax

D = 4096
HEADS = 32
HD = 64
QB = 64
L_CMP = 32
TOP = 8
SEQS = 4
SEQ_LEN = 2048
N_TP = 8


def draw_tokens(key, part):
    base = jnp.clip(jax.random.normal(key, (SEQ_LEN, SEQS, D), jnp.float32), -6.0, 6.0)
    return base.astype(jnp.bfloat16)


def draw_chosen(key, part):
    block_count = SEQ_LEN // QB
    noise = jax.random.randint(key, (SEQS, HEADS, block_count, block_count), 0, 1024)
    favored = jax.random.randint(jax.random.fold_in(key, 1), (SEQS, HEADS, 1, block_count), 0, 4)
    priority = noise + (favored == 0).astype(jnp.int32) * 2048
    query_blk = jnp.arange(block_count)[:, None]
    key_blk = jnp.arange(block_count)[None, :]
    forced = (key_blk == query_blk) | (key_blk == query_blk - 1) | (key_blk == 0)
    priority = jnp.where(forced, 8192, priority)
    priority = jnp.where(key_blk <= query_blk, priority + 1, 0)
    ranking = priority * block_count + (block_count - 1 - key_blk)
    top_scores, top_index = lax.top_k(ranking, TOP)
    live_slot = jnp.arange(TOP)[None, :] < jnp.minimum(jnp.arange(block_count) + 1, TOP)[:, None]
    return jnp.where(live_slot[None, None], top_index, -1).astype(jnp.int32)


def block_levels(key, shape, pieces, smallest, largest):
    loudness = 1.0
    for axis_at, blocks in pieces:
        heights = jax.random.uniform(jax.random.fold_in(jax.random.fold_in(key, 6), axis_at), (blocks,), jnp.float32, smallest / len(pieces), largest / len(pieces))
        loudness = loudness * jnp.repeat(jnp.exp(heights), shape[axis_at] // blocks).reshape((-1,) + (1,) * (len(shape) - 1 - axis_at))
    return loudness


def length_profile(amount, total, reach, skew):
    weights = [(1 << 20) // math.isqrt(rank ** skew) + 1 for rank in range(2, amount + 1)]
    rest, counts = total - reach - (amount - 1), [1] * (amount - 1)
    while rest > 0:
        candidates = [i for i in range(amount - 1) if counts[i] < reach]
        mass, remaining = sum([weights[i] for i in candidates]), rest
        for i in candidates:
            more = min(reach - counts[i], max(1, remaining * weights[i] // mass), rest)
            counts[i] = counts[i] + more
            rest = rest - more
    return np.array([reach] + counts)


def uneven_parts(rng, number_of, total, most, lean):
    if number_of == 2:
        one = jax.random.randint(rng, (), max(1, total - most), min(most, total - 1) + 1)
        return jnp.stack([one, total - one])
    sizes = jnp.asarray(length_profile(number_of, total, most, lean), jnp.int32)
    couples = (number_of - 1) // 2
    giver, sink = sizes[1:1 + 2 * couples:2], sizes[2:2 + 2 * couples:2]
    slack = jnp.minimum(giver - 1, most - sink)
    moved = jax.random.randint(jax.random.fold_in(rng, 1), (couples,), 0, 1 << 20) % (slack + 1)
    sizes = sizes.at[1:1 + 2 * couples:2].set(giver - moved).at[2:2 + 2 * couples:2].set(sink + moved)
    return sizes[jax.random.permutation(jax.random.fold_in(rng, 2), number_of)]


def scatter_about(own_key, dims, width, bound, split=(), dtype=jnp.bfloat16):
    result = jax.random.normal(own_key, dims, jnp.float32) * width
    if len(split) > 0:
        result = block_levels(own_key, dims, split, -0.22, 0.18) * result
    return jnp.clip(result, min=-bound, max=bound).astype(dtype)


def setup_inputs(seed: int = 0, part: int = 0) -> dict:
    keys = jax.random.split(jax.random.key(seed), 10)
    part_splits = jax.random.split(jax.random.fold_in(keys[9], part), 10)
    return {
        "tokens": draw_tokens(jax.random.fold_in(jax.random.fold_in(keys[9], part), 71), part),
        "lengths": uneven_parts(part_splits[1], SEQS, SEQS * SEQ_LEN * 3 // 8, SEQ_LEN, 2).astype(jnp.int32),
        "chosen": draw_chosen(jax.random.fold_in(jax.random.fold_in(keys[9], part), 71), part),
        "w_query": scatter_about(keys[3], (D, HEADS * HD), D ** -0.5, 0.09375, ((1, 8),)),
        "w_key": scatter_about(keys[4], (D, HEADS * HD), D ** -0.5, 0.09375, ((1, 8),)),
        "w_value": scatter_about(keys[5], (D, HEADS * HD), D ** -0.5, 0.09375, ((1, 8),)),
        "w_gate": scatter_about(keys[6], (D, 2, HEADS), D ** -0.5, 0.09375, ((2, 8),)),
        "pool_weights": scatter_about(keys[7], (2, L_CMP, HD), L_CMP ** -0.5, 1.0, (), jnp.float32),
        "w_out": scatter_about(keys[8], (HEADS * HD, D), (HEADS * HD // 16) ** -0.5, 0.5, ((1, 8),)),
    }


LOW_FILL = -1e30


def rounded(value):
    return lax.optimization_barrier(value.astype(jnp.bfloat16)).astype(jnp.float32)


def head_attend(queries, key_rows, value_rows, chosen, pool_weights, lengths):
    seq_len, seq_count, head_dim = queries.shape
    score_scale = head_dim ** -0.5
    query_pos = jnp.arange(seq_len)
    cmp_count = seq_len // L_CMP
    key_pooled = rounded((key_rows.reshape(cmp_count, L_CMP, seq_count, head_dim) * pool_weights[0][None, :, None, :]).sum(1))
    val_pooled = rounded((value_rows.reshape(cmp_count, L_CMP, seq_count, head_dim) * pool_weights[1][None, :, None, :]).sum(1))
    cmp_end = jnp.arange(cmp_count) * L_CMP + L_CMP - 1
    scores = jnp.einsum('qsd,csd->sqc', queries, key_pooled) * score_scale
    usable = (cmp_end[None, None, :] <= query_pos[None, :, None]) & (cmp_end[None, None, :] < lengths[:, None, None])
    row_top = jnp.max(jnp.where(usable, scores, LOW_FILL), axis=-1, keepdims=True)
    weights = jnp.where(usable, jnp.exp(scores - row_top), 0.0)
    totals = jnp.sum(weights, axis=-1)
    pooled_out = jnp.einsum('sqc,csd->sqd', rounded(weights), val_pooled) / jnp.where(totals > 0, totals, 1.0)[..., None]
    block_count = seq_len // QB
    key_table = key_rows.reshape(block_count, QB, seq_count, head_dim).transpose(2, 0, 1, 3)
    val_table = value_rows.reshape(block_count, QB, seq_count, head_dim).transpose(2, 0, 1, 3)
    clipped = jnp.maximum(chosen, 0)
    index = clipped[:, :, :, None, None]
    key_sel = jnp.take_along_axis(key_table[:, None], index, axis=2).reshape(seq_count, block_count, TOP * QB, head_dim)
    val_sel = jnp.take_along_axis(val_table[:, None], index, axis=2).reshape(seq_count, block_count, TOP * QB, head_dim)
    query_blocks = queries.transpose(1, 0, 2).reshape(seq_count, block_count, QB, head_dim)
    scores = jnp.einsum('sbqd,sbkd->sbqk', query_blocks, key_sel) * score_scale
    key_pos = (clipped[..., None] * QB + jnp.arange(QB)).reshape(seq_count, block_count, TOP * QB)
    live_key = jnp.repeat(chosen >= 0, QB, axis=-1)
    block_pos = query_pos.reshape(block_count, QB)
    usable = live_key[:, :, None, :] & (key_pos[:, :, None, :] <= block_pos[None, :, :, None]) & (key_pos[:, :, None, :] < lengths[:, None, None, None])
    row_top = jnp.max(jnp.where(usable, scores, LOW_FILL), axis=-1, keepdims=True)
    weights = jnp.where(usable, jnp.exp(scores - row_top), 0.0)
    totals = jnp.sum(weights, axis=-1)
    picked_out = jnp.einsum('sbqk,sbkd->sbqd', rounded(weights), val_sel) / jnp.where(totals > 0, totals, 1.0)[..., None]
    return pooled_out, picked_out.reshape(seq_count, seq_len, head_dim)


def reference(tokens, lengths, chosen, w_query, w_key, w_value, w_gate, pool_weights, w_out):
    seq_len, seq_count, model_width = tokens.shape
    head_count = w_query.shape[1] // HD
    flat_rows = tokens.reshape(seq_len * seq_count, model_width)

    def project(weight):
        product = jnp.dot(flat_rows, weight, preferred_element_type=jnp.float32)
        return rounded(product).reshape(seq_len, seq_count, head_count, HD).transpose(2, 0, 1, 3)

    queries = project(w_query)
    key_rows = project(w_key)
    value_rows = project(w_value)
    gate_values = jax.nn.sigmoid(jnp.dot(flat_rows, w_gate.reshape(model_width, 2 * head_count), preferred_element_type=jnp.float32))
    gate_values = gate_values.reshape(seq_len, seq_count, 2, head_count)

    def one_head(inputs):
        return head_attend(inputs[0], inputs[1], inputs[2], inputs[3], pool_weights, lengths)

    pooled_out, picked_out = lax.map(one_head, (queries, key_rows, value_rows, chosen.transpose(1, 0, 2, 3)))
    combined = gate_values[:, :, 0, :, None] * pooled_out.transpose(2, 1, 0, 3) + gate_values[:, :, 1, :, None] * picked_out.transpose(2, 1, 0, 3)
    live = jnp.arange(seq_len)[:, None] < lengths[None, :]
    attended = jnp.where(live[:, :, None, None], combined, 0.0).astype(jnp.bfloat16).reshape(seq_len * seq_count, head_count * HD)
    part_width = head_count * HD // N_TP
    summed = jnp.zeros((seq_len * seq_count, model_width), jnp.float32)
    for shard in range(N_TP):
        product = jnp.dot(attended[:, shard * part_width:(shard + 1) * part_width], w_out[shard * part_width:(shard + 1) * part_width], preferred_element_type=jnp.float32)
        summed = summed + rounded(product)
    return summed.astype(jnp.bfloat16).reshape(seq_len, seq_count, model_width)
```

```python
import jax
import jax.numpy as jnp
from jax import lax
from jax.experimental import pallas as pl
from jax.experimental.pallas import tpu as pltpu
from jax.sharding import PartitionSpec as P

HD = 64
QB = 64
L_CMP = 32
NEG = -1e30
BF = jnp.bfloat16
F32 = jnp.float32
MESH = pl.DeviceIdType.MESH

ROWS = 128
AUX = 16
MSG = 3 * HD + AUX
LAST = (15, 11, 7, 5)
PLACE = (
    (13, 9, 11, 15),
    (6, 4, 7, 5),
    (3, 4, 2, 12),
    (3, 1, 0, 2),
)
RANK_ORDER = (0, 1, 2, 3)
TILE = 256


def iota(shape, dim):
    return lax.broadcasted_iota(jnp.int32, shape, dim)


def nt(a, b):
    return lax.dot_general(a, b, (((1,), (1,)), ((), ())), preferred_element_type=F32)


def nn(a, b):
    return jnp.dot(a, b, preferred_element_type=F32)


def kernel(
    n_kv, n_tp, n_seq, n_head,
    tok_hbm, len_ref, chosen_rows, wq_hbm, wk_hbm, wv_hbm, wg_ref, pw_ref, wo_hbm,
    out_ref,
    tok, w_buf, wo, sel_t, send, recv, k_ext, q_ext, v_all, pool_in, o_stage, a_buf, x_buf, y_buf, o_buf,
    load_sem, q_send, q_recv, o_send, o_recv, g_send, g_recv, y_send, y_recv,
):
    me = lax.axis_index("kv")
    tp = lax.axis_index("tp")
    chips = n_tp // 2
    core = lax.rem(tp, 2)
    chip = tp // 2
    right = lax.rem(chip + 1, chips) * 2 + core
    left = lax.rem(chip + chips - 1, chips) * 2 + core
    far = lax.rem(chip + 2, chips) * 2 + core
    partner = chip * 2 + 1 - core

    barrier = pltpu.get_barrier_semaphore()
    for step in range(1, n_kv):
        pl.semaphore_signal(
            barrier, inc=1, device_id={"kv": lax.rem(me + step, n_kv)}, device_id_type=MESH
        )
    for step in range(1, n_tp):
        pl.semaphore_signal(
            barrier, inc=1, device_id={"tp": lax.rem(tp + step, n_tp)}, device_id_type=MESH
        )

    loads = [
        pltpu.make_async_copy(tok_hbm, tok, load_sem.at[0]),
        pltpu.make_async_copy(wk_hbm, w_buf.at[0], load_sem.at[1]),
        pltpu.make_async_copy(wv_hbm, w_buf.at[1], load_sem.at[2]),
        pltpu.make_async_copy(wq_hbm, w_buf.at[2], load_sem.at[3]),
        pltpu.make_async_copy(wo_hbm, wo, load_sem.at[4]),
    ]
    for copy in loads:
        copy.start()

    lens = [len_ref[s] for s in range(n_seq)]
    ranks = []
    for s in range(n_seq):
        rank = jnp.int32(0)
        for o in range(n_seq):
            if o != s:
                ahead = (lens[o] >= lens[s]) if o < s else (lens[o] > lens[s])
                rank = rank + ahead.astype(jnp.int32)
        ranks.append(rank)
    seq_of, len_of = [], []
    for r in range(n_seq):
        seq, length = jnp.int32(0), jnp.int32(0)
        for s in range(n_seq):
            hit = (ranks[s] == r).astype(jnp.int32)
            seq = seq + hit * s
            length = length + hit * lens[s]
        seq_of.append(seq)
        len_of.append(length)

    total = ROWS * n_seq
    row = iota((total, ROWS), 0)
    col = iota((total, ROWS), 1)
    for r in range(n_seq):
        hit = row == col * n_seq + seq_of[r]
        sel_t[:, r * ROWS : (r + 1) * ROWS] = jnp.where(hit, 1.0, 0.0).astype(BF)

    loads[0].wait()
    flat = tok[...].reshape(total, tok.shape[2])
    for part, slot, base in ((1, 0, HD), (2, 1, 2 * HD), (3, 2, 0)):
        loads[part].wait()
        made = nn(flat, w_buf[slot]).astype(BF).T
        placed = nn(made, sel_t[...])
        if base == 0:
            placed = placed * HD**-0.5
        placed = placed.astype(BF)
        for r in range(n_seq):
            for h in range(n_head):
                send[r * n_head + h, base : base + HD, :] = placed[
                    h * HD : (h + 1) * HD, r * ROWS : (r + 1) * ROWS
                ]
    gates = jax.nn.sigmoid(nt(flat, wg_ref[...]))
    gate_hi = gates.astype(BF)
    gate_lo = (gates - gate_hi.astype(F32)).astype(BF)
    gate_hi = nn(gate_hi.T, sel_t[...])
    gate_lo = nn(gate_lo.T, sel_t[...])
    for r in range(n_seq):
        cols = slice(r * ROWS, (r + 1) * ROWS)
        for h in range(n_head):
            picked = chosen_rows[seq_of[r], h]
            aux = jnp.concatenate(
                [
                    gate_hi[h : h + 1, cols],
                    gate_hi[n_head + h : n_head + h + 1, cols],
                    gate_lo[h : h + 1, cols],
                    gate_lo[n_head + h : n_head + h + 1, cols],
                    jnp.zeros((4, ROWS), F32),
                    picked,
                ],
                axis=0,
            )
            send[r * n_head + h, 3 * HD :, :] = aux.astype(BF)

    pl.semaphore_wait(barrier, n_kv - 1 + n_tp - 1)

    def message(r, h):
        return pltpu.make_async_remote_copy(
            src_ref=send.at[r * n_head + h],
            dst_ref=recv.at[r, me],
            send_sem=q_send.at[r * n_head + h],
            recv_sem=q_recv.at[r, me],
            device_id={"kv": jnp.int32(PLACE[r][h])},
            device_id_type=MESH,
        )

    def arrival(r, j):
        return pltpu.make_async_remote_copy(
            src_ref=send.at[0],
            dst_ref=recv.at[r, j],
            send_sem=q_send.at[0],
            recv_sem=q_recv.at[r, j],
            device_id={"kv": jnp.int32(0)},
            device_id_type=MESH,
        )

    for r in RANK_ORDER:
        for h in range(n_head):
            there = PLACE[r][h]

            @pl.when((me <= LAST[r]) & (me != there))
            def _():
                message(r, h).start()

            if there <= LAST[r]:

                @pl.when(me == there)
                def _():
                    recv[r, there] = send[r * n_head + h]

    def returned(r, h_here, j):
        return pltpu.make_async_remote_copy(
            src_ref=o_stage.at[r, j],
            dst_ref=a_buf.at[r, h_here],
            send_sem=o_send.at[r, j],
            recv_sem=o_recv.at[r, h_here],
            device_id={"kv": jnp.int32(j)},
            device_id_type=MESH,
        )

    def attend(r):
        shards = LAST[r] + 1
        span = shards * ROWS
        length = len_of[r]
        head = jnp.int32(0)
        for h in range(n_head):
            head = head + (me == PLACE[r][h]).astype(jnp.int32) * h

        pw_keys = jnp.concatenate([pw_ref[0].T] * (ROWS // L_CMP), axis=1)
        pw_vals = jnp.concatenate([pw_ref[1].T] * (ROWS // L_CMP), axis=1)
        weight = jnp.concatenate([pw_keys, pw_vals], axis=0)
        lane_blk = iota((ROWS, ROWS), 0) // L_CMP
        lane_col = iota((ROWS, ROWS), 1)

        def prepare(j, pooled):
            @pl.when(j != me)
            def _():
                arrival(r, j).wait_recv()

            cols = pl.ds(pl.multiple_of(j * ROWS, ROWS), ROWS)
            q_ext[0:HD, cols] = recv[r, j, 0:HD, :]
            k_ext[0:HD, cols] = recv[r, j, HD : 2 * HD, :]
            v_all[:, cols] = recv[r, j, 2 * HD : 3 * HD, :]
            picks = recv[r, j, 3 * HD : MSG, :].astype(F32)
            blocks = iota((32, ROWS), 0).astype(F32)
            hit = blocks == picks[8:9]
            for t in range(1, 8):
                hit = hit | (blocks == picks[8 + t : 9 + t])
            q_ext[HD : HD + 32, cols] = jnp.where(hit, 0.0, NEG).astype(BF)
            one_row = (iota((32, ROWS), 0) == 0).astype(F32)
            q_ext[HD + 32 :, cols] = one_row.astype(BF)
            key = j * ROWS + iota((32, ROWS), 1)
            k_ext[HD : HD + 32, cols] = (iota((32, ROWS), 0) == key // QB).astype(F32).astype(BF)
            k_ext[HD + 32 :, cols] = jnp.where(key >= length, one_row * NEG, 0.0).astype(BF)
            prod = recv[r, j, HD : 3 * HD, :].astype(F32) * weight
            hi = prod.astype(BF)
            lo = (prod - hi.astype(F32)).astype(BF)
            group = jnp.where(lane_col == j * (ROWS // L_CMP) + lane_blk, 1.0, 0.0).astype(BF)
            both = nn(jnp.concatenate([hi, lo], axis=0), group)
            return pooled + both[: 2 * HD] + both[2 * HD :]

        pooled = lax.fori_loop(0, shards, prepare, jnp.zeros((2 * HD, ROWS), F32)).astype(BF)
        key_pooled = jnp.concatenate([pooled[:HD], jnp.zeros((HD, ROWS), BF)], axis=0)
        val_pooled = pooled[HD:]
        for t in range(span // TILE):
            lo, hi = t * TILE, (t + 1) * TILE
            q = q_ext[:, lo:hi].T
            scores = nn(q, k_ext[:, :hi])
            edge = jnp.where(
                iota((TILE, TILE), 1) <= iota((TILE, TILE), 0), scores[:, lo:hi], NEG
            )
            scores = edge if t == 0 else jnp.concatenate([scores[:, :lo], edge], axis=1)
            top = jnp.max(scores, axis=1, keepdims=True)
            e = jnp.exp(scores - top)
            tot = jnp.sum(e, axis=1, keepdims=True)
            picked_out = nt(e.astype(BF), v_all[:, :hi]) / tot

            scores = nn(q, key_pooled)
            pos = lo + iota((TILE, ROWS), 0)
            end = iota((TILE, ROWS), 1) * L_CMP + (L_CMP - 1)
            usable = (end <= pos) & (end < length)
            top = jnp.max(jnp.where(usable, scores, NEG), axis=1, keepdims=True)
            e = jnp.where(usable, jnp.exp(jnp.where(usable, scores, NEG) - top), 0.0)
            tot = jnp.sum(e, axis=1, keepdims=True)
            pooled_out = nt(e.astype(BF), val_pooled) / jnp.where(tot > 0, tot, 1.0)

            both = jnp.concatenate([pooled_out, picked_out], axis=1).T
            for i in range(TILE // ROWS):
                j = t * (TILE // ROWS) + i
                g = recv[r, j, 3 * HD : MSG, :].astype(F32)
                part = both[:, i * ROWS : (i + 1) * ROWS]
                mix = (g[0:1] + g[2:3]) * part[:HD] + (g[1:2] + g[3:4]) * part[HD:]
                alive = j * ROWS + iota((HD, ROWS), 1) < length
                o_stage[r, j] = jnp.where(alive, mix, 0.0).astype(BF)

                @pl.when(me != j)
                def _():
                    returned(r, head, j).start()

                @pl.when(me == j)
                def _():
                    a_buf[r, head] = o_stage[r, j]

    def placed_here(r):
        here = me == PLACE[r][0]
        for h in range(1, n_head):
            here = here | (me == PLACE[r][h])
        return here

    for r in RANK_ORDER:

        @pl.when(placed_here(r))
        def _():
            attend(r)

    half = ROWS // 2
    lower, upper = pl.ds(0, half), pl.ds(half, half)

    def hop(r, block, rows, to, n):
        ref = x_buf.at[r, block] if rows is None else x_buf.at[r, block, rows]
        return pltpu.make_async_remote_copy(
            src_ref=ref,
            dst_ref=ref,
            send_sem=g_send.at[r, n],
            recv_sem=g_recv.at[r, n],
            device_id={"tp": to},
            device_id_type=MESH,
        )

    def sends(r):
        return [
            hop(r, tp, lower, right, 0),
            hop(r, tp, upper, right, 1),
            hop(r, tp, upper, left, 2),
            hop(r, tp, lower, left, 3),
            hop(r, left, lower, right, 4),
            hop(r, right, upper, left, 5),
            hop(r, tp, None, partner, 6),
            hop(r, left, None, partner, 7),
            hop(r, right, None, partner, 8),
            hop(r, far, None, partner, 9),
        ]

    def other(t):
        return t + 1 - 2 * lax.rem(t, 2)

    def receipts(r):
        return [
            hop(r, left, lower, left, 0),
            hop(r, left, upper, left, 1),
            hop(r, right, upper, right, 2),
            hop(r, right, lower, right, 3),
            hop(r, far, lower, left, 4),
            hop(r, far, upper, right, 5),
            hop(r, other(tp), None, partner, 6),
            hop(r, other(left), None, partner, 7),
            hop(r, other(right), None, partner, 8),
            hop(r, other(far), None, partner, 9),
        ]

    rows_each = ROWS // n_tp
    width = wo.shape[1]

    def column_copy(r, to):
        return pltpu.make_async_remote_copy(
            src_ref=y_buf.at[r, pl.ds(pl.multiple_of(to * rows_each, rows_each), rows_each)],
            dst_ref=o_buf.at[r, :, pl.ds(pl.multiple_of(tp * width, width), width)],
            send_sem=y_send.at[r, to],
            recv_sem=y_recv.at[r, tp],
            device_id={"tp": to},
            device_id_type=MESH,
        )

    def column_arrival(r, source):
        return pltpu.make_async_remote_copy(
            src_ref=y_buf.at[r, pl.ds(0, rows_each)],
            dst_ref=o_buf.at[r, :, pl.ds(pl.multiple_of(source * width, width), width)],
            send_sem=y_send.at[r, source],
            recv_sem=y_recv.at[r, source],
            device_id={"tp": source},
            device_id_type=MESH,
        )

    loads[4].wait()

    def spread(r):
        for h in range(n_head):

            @pl.when(me != PLACE[r][h])
            def _():
                pltpu.make_async_remote_copy(
                    src_ref=o_stage.at[r, 0],
                    dst_ref=a_buf.at[r, h],
                    send_sem=o_send.at[r, 0],
                    recv_sem=o_recv.at[r, h],
                    device_id={"kv": jnp.int32(PLACE[r][h])},
                    device_id_type=MESH,
                ).wait_recv()

        x_buf[r, tp] = a_buf[r].reshape(n_head * HD, ROWS).T
        out, into = sends(r), receipts(r)
        for n in (0, 2, 1, 3, 6):
            out[n].start()
        into[0].wait_recv()
        out[4].start()
        into[2].wait_recv()
        out[5].start()
        into[1].wait_recv()
        out[7].start()
        into[3].wait_recv()
        out[8].start()
        into[4].wait_recv()
        into[5].wait_recv()
        out[9].start()
        for n in (6, 7, 8, 9):
            into[n].wait_recv()
        rows = jnp.concatenate([x_buf[r, g] for g in range(n_tp)], axis=1)
        y_buf[r] = nn(rows, wo[...]).astype(BF)
        for step in range(1, n_tp):
            column_copy(r, lax.rem(tp + step, n_tp)).start()
        mine = pl.ds(pl.multiple_of(tp * rows_each, rows_each), rows_each)
        o_buf[r, :, pl.ds(pl.multiple_of(tp * width, width), width)] = y_buf[r, mine]

    for r in RANK_ORDER:

        @pl.when(me <= LAST[r])
        def _():
            spread(r)

        @pl.when(me > LAST[r])
        def _():
            o_buf[r] = jnp.zeros(o_buf.shape[1:], BF)

    for r in range(n_seq):

        @pl.when(me <= LAST[r])
        def _():
            for step in range(1, n_tp):
                column_arrival(r, lax.rem(tp + step, n_tp)).wait_recv()

    many = rows_each * n_seq
    want = iota((many, many), 0)
    have = iota((many, many), 1)
    pick = jnp.zeros((many, many), F32)
    for r in range(n_seq):
        hit = (have == r * rows_each + want // n_seq) & (lax.rem(want, n_seq) == seq_of[r])
        pick = jnp.where(hit, 1.0, pick)
    pick = pick.astype(BF)
    for c in range(n_tp):
        cols = slice(c * width, (c + 1) * width)
        rows = o_buf[:, :, cols].reshape(many, width)
        out_ref[:, cols] = nn(pick, rows).astype(BF)

    for r in range(n_seq):
        for h in range(n_head):

            @pl.when((me <= LAST[r]) & (me != PLACE[r][h]))
            def _():
                message(r, h).wait_send()

        @pl.when(placed_here(r))
        def _():
            for j in range(LAST[r] + 1):

                @pl.when(me != j)
                def _():
                    returned(r, 0, j).wait_send()

        @pl.when(me <= LAST[r])
        def _():
            for copy in sends(r):
                copy.wait_send()
            for step in range(1, n_tp):
                column_copy(r, lax.rem(tp + step, n_tp)).wait_send()


def body(tokens, lengths, chosen, w_query, w_key, w_value, w_gate, pool_weights, w_out):
    rows, n_seq, depth = tokens.shape
    n_head = w_query.shape[1] // HD
    n_kv, n_tp = lax.axis_size("kv"), lax.axis_size("tp")
    blocks = chosen.shape[2]
    picks = jnp.repeat(jnp.swapaxes(chosen, 2, 3), rows // blocks, axis=3).astype(F32)
    gate_rows = jnp.transpose(w_gate, (1, 2, 0)).reshape(2 * n_head, depth)
    width = w_out.shape[1]
    total = rows * n_seq
    vmem = pl.BlockSpec(memory_space=pltpu.VMEM)
    hbm = pl.BlockSpec(memory_space=pl.ANY)
    dma = pltpu.SemaphoreType.DMA
    full = n_kv * rows

    def whole(*refs):
        kernel(n_kv, n_tp, n_seq, n_head, *refs)

    out = pl.pallas_call(
        whole,
        out_shape=jax.ShapeDtypeStruct((total // n_tp, n_tp * width), BF),
        in_specs=[
            hbm, pl.BlockSpec(memory_space=pltpu.SMEM), vmem, hbm, hbm, hbm, vmem, vmem, hbm,
        ],
        out_specs=vmem,
        scratch_shapes=[
            pltpu.VMEM((rows, n_seq, depth), BF),
            pltpu.VMEM((3, depth, n_head * HD), BF),
            pltpu.VMEM(w_out.shape, BF),
            pltpu.VMEM((total, total), BF),
            pltpu.VMEM((n_seq * n_head, MSG, rows), BF),
            pltpu.VMEM((n_seq, n_kv, MSG, rows), BF),
            pltpu.VMEM((128, full), BF),
            pltpu.VMEM((128, full), BF),
            pltpu.VMEM((HD, full), BF),
            pltpu.VMEM((8, 128), F32),
            pltpu.VMEM((n_seq, n_kv, HD, rows), BF),
            pltpu.VMEM((n_seq, n_head, HD, rows), BF),
            pltpu.VMEM((n_seq, n_tp, rows, n_head * HD), BF),
            pltpu.VMEM((n_seq, rows, width), BF),
            pltpu.VMEM((n_seq, rows // n_tp, n_tp * width), BF),
            dma((5,)),
            dma((n_seq * n_head,)),
            dma((n_seq, n_kv)),
            dma((n_seq, n_kv)),
            dma((n_seq, n_head)),
            dma((n_seq, 10)),
            dma((n_seq, 10)),
            dma((n_seq, n_tp)),
            dma((n_seq, n_tp)),
        ],
        compiler_params=pltpu.CompilerParams(
            collective_id=0, has_side_effects=True, vmem_limit_bytes=60 * 2**20
        ),
    )(tokens, lengths, picks, w_query, w_key, w_value, gate_rows, pool_weights, w_out)
    return out.reshape(rows // n_tp, n_seq, n_tp * width)


def solution(mesh):
    placed = (
        P("kv", "grp", None),
        P("grp"),
        P("grp", "tp", "kv", None),
        P(None, "tp"),
        P(None, "tp"),
        P(None, "tp"),
        P(None, None, "tp"),
        P(),
        P(None, "tp"),
    )
    return jax.shard_map(
        body, mesh=mesh, in_specs=placed, out_specs=P(("kv", "tp"), "grp", None), check_vma=False
    )
```

```python
import jax
import jax.numpy as jnp
from jax import lax
from jax.experimental import pallas as pl
from jax.experimental.pallas import tpu as pltpu
from jax.sharding import PartitionSpec as P

HD = 64
QB = 64
L_CMP = 32
NEG = -1e30
BF = jnp.bfloat16
F32 = jnp.float32
MESH = pl.DeviceIdType.MESH

ROWS = 128
AUX = 16
MSG = 3 * HD + AUX
KEYS, VALS, QUER, EXTRA = 0, HD, 2 * HD, 3 * HD
LAST = (15, 11, 7, 5)
PLACE = (
    (9, 11, 12, 13),
    (4, 5, 6, 7),
    (3, 4, 1, 2),
    (2, 3, 1, 5),
)
RANK_ORDER = (3, 2, 1, 0)
TILE = 256
SHARDS = LAST[0] + 1
PAIRED = sorted({p for places in PLACE for p in places})


def returns_to(i, j):
    return any(i in PLACE[r] and j <= LAST[r] for r in range(len(PLACE)))


def sends_to(i, j):
    asked = any(j in PLACE[r] and i <= LAST[r] for r in range(len(PLACE)))
    return asked or returns_to(i, j)


def any_of(me, places):
    here = me < 0
    for p in places:
        here = here | (me == p)
    return here


def iota(shape, dim):
    return lax.broadcasted_iota(jnp.int32, shape, dim)


def nt(a, b):
    return lax.dot_general(a, b, (((1,), (1,)), ((), ())), preferred_element_type=F32)


def nn(a, b):
    return jnp.dot(a, b, preferred_element_type=F32)


def kernel(
    n_kv, n_tp, n_seq, n_head,
    tok_hbm, len_hbm, chosen_hbm, wq_hbm, wk_hbm, wv_hbm, wg_hbm, pw_hbm, wo_hbm,
    out_ref,
    tok, flat, w_buf, wg, pw_ref, wo, len_ref, chosen_ref,
    sel_t, send, recv, k_ext, q_ext, v_all, weight, pool_sum, o_stage, a_buf, x_buf, y_buf, o_buf,
    load_sem, k_send, k_recv, q_send, q_recv, o_send, o_recv, g_send, g_recv, y_send, y_recv,
    ready_kv, ready_tp,
):
    me = lax.axis_index("kv")
    tp = lax.axis_index("tp")
    chips = n_tp // 2
    core = lax.rem(tp, 2)
    chip = tp // 2
    right = lax.rem(chip + 1, chips) * 2 + core
    left = lax.rem(chip + chips - 1, chips) * 2 + core
    far = lax.rem(chip + 2, chips) * 2 + core
    partner = chip * 2 + 1 - core

    barrier = pltpu.get_barrier_semaphore()
    for j in range(n_kv):

        @pl.when(me < j)
        def _():
            pl.semaphore_signal(
                barrier, inc=1, device_id={"kv": jnp.int32(j)}, device_id_type=MESH
            )

    for t in range(n_tp):

        @pl.when(tp > t)
        def _():
            pl.semaphore_signal(
                barrier, inc=1, device_id={"tp": jnp.int32(t)}, device_id_type=MESH
            )

    loads = [
        pltpu.make_async_copy(len_hbm, len_ref, load_sem.at[0]),
        pltpu.make_async_copy(tok_hbm, tok, load_sem.at[1]),
        pltpu.make_async_copy(wk_hbm, w_buf.at[0], load_sem.at[2]),
        pltpu.make_async_copy(wv_hbm, w_buf.at[1], load_sem.at[3]),
        pltpu.make_async_copy(wq_hbm, w_buf.at[2], load_sem.at[4]),
        pltpu.make_async_copy(wg_hbm, wg, load_sem.at[5]),
        pltpu.make_async_copy(chosen_hbm, chosen_ref, load_sem.at[6]),
        pltpu.make_async_copy(pw_hbm, pw_ref, load_sem.at[7]),
        pltpu.make_async_copy(wo_hbm, wo, load_sem.at[8]),
    ]
    for copy in loads:
        copy.start()
    told = me + n_tp - 1 - tp

    @pl.when(told > 0)
    def _():
        pl.semaphore_wait(barrier, told)

    for i in range(n_kv):
        later = [j for j in range(i + 1, n_kv) if sends_to(i, j)]

        @pl.when(any_of(me, later))
        def _():
            pl.semaphore_signal(
                ready_kv.at[me], inc=1, device_id={"kv": jnp.int32(i)}, device_id_type=MESH
            )

    for t in range(n_tp):

        @pl.when(tp < t)
        def _():
            pl.semaphore_signal(
                ready_tp.at[tp], inc=1, device_id={"tp": jnp.int32(t)}, device_id_type=MESH
            )

    loads[0].wait()

    lens = [len_ref[s] for s in range(n_seq)]
    ranks = []
    for s in range(n_seq):
        rank = jnp.int32(0)
        for o in range(n_seq):
            if o != s:
                ahead = (lens[o] >= lens[s]) if o < s else (lens[o] > lens[s])
                rank = rank + ahead.astype(jnp.int32)
        ranks.append(rank)
    seq_of, len_of = [], []
    for r in range(n_seq):
        seq, length = jnp.int32(0), jnp.int32(0)
        for s in range(n_seq):
            hit = (ranks[s] == r).astype(jnp.int32)
            seq = seq + hit * s
            length = length + hit * lens[s]
        seq_of.append(seq)
        len_of.append(length)

    total = ROWS * n_seq
    row = iota((total, ROWS), 0)
    col = iota((total, ROWS), 1)
    for r in range(n_seq):
        hit = row == col * n_seq + seq_of[r]
        sel_t[:, r * ROWS : (r + 1) * ROWS] = jnp.where(hit, 1.0, 0.0).astype(BF)

    loads[1].wait()
    flat[...] = tok[...].reshape(flat.shape)

    def project(slot, base):
        loads[2 + slot].wait()
        made = nn(flat[...], w_buf[slot]).astype(BF).T
        placed = nn(made, sel_t[...])
        if base == QUER:
            placed = placed * HD**-0.5
        placed = placed.astype(BF)
        for r in range(n_seq):
            for h in range(n_head):
                send[r * n_head + h, base : base + HD, :] = placed[
                    h * HD : (h + 1) * HD, r * ROWS : (r + 1) * ROWS
                ]

    def extras():
        loads[5].wait()
        loads[6].wait()
        gates = jax.nn.sigmoid(nt(wg[...].reshape(2 * n_head, wg.shape[2]), flat[...]))
        gate_hi = gates.astype(BF)
        gate_lo = (gates - gate_hi.astype(F32)).astype(BF)
        gate_rows = nn(jnp.concatenate([gate_hi, gate_lo], axis=0), sel_t[...])
        n_blk, top = chosen_ref.shape[2:]
        slot = iota((top, ROWS), 0)
        blk = iota((top, ROWS), 1) // (ROWS // n_blk)
        for r in range(n_seq):
            cols = slice(r * ROWS, (r + 1) * ROWS)
            for h in range(n_head):
                picked = jnp.zeros((top, ROWS), jnp.int32)
                for b in range(n_blk):
                    for t in range(top):
                        at = (slot == t) & (blk == b)
                        picked = jnp.where(at, chosen_ref[seq_of[r], h, b, t], picked)
                kinds = [
                    gate_rows[g * n_head + h : g * n_head + h + 1, cols] for g in range(4)
                ]
                rest = jnp.zeros((AUX - top - 4, ROWS), F32)
                aux = jnp.concatenate([*kinds, rest, picked.astype(F32)], axis=0)
                send[r * n_head + h, EXTRA:, :] = aux.astype(BF)

    pair_rows = pl.ds(0, QUER)
    query_rows = pl.ds(QUER, MSG - QUER)

    def message(r, h, queries):
        rows = query_rows if queries else pair_rows
        return pltpu.make_async_remote_copy(
            src_ref=send.at[r * n_head + h, rows],
            dst_ref=recv.at[r, me, rows],
            send_sem=(q_send if queries else k_send).at[r * n_head + h],
            recv_sem=(q_recv if queries else k_recv).at[r, me],
            device_id={"kv": jnp.int32(PLACE[r][h])},
            device_id_type=MESH,
        )

    def arrival(r, j, queries):
        rows = query_rows if queries else pair_rows
        return pltpu.make_async_remote_copy(
            src_ref=send.at[0, rows],
            dst_ref=recv.at[r, j, rows],
            send_sem=(q_send if queries else k_send).at[0],
            recv_sem=(q_recv if queries else k_recv).at[r, j],
            device_id={"kv": jnp.int32(0)},
            device_id_type=MESH,
        )

    asked = set()

    def send_rank(r, queries):
        for h in range(n_head):
            there = PLACE[r][h]
            if there not in asked:
                asked.add(there)

                @pl.when(any_of(me, [i for i in range(there) if sends_to(i, there)]))
                def _():
                    pl.semaphore_wait(ready_kv.at[there], 1)

            @pl.when((me <= LAST[r]) & (me != there))
            def _():
                message(r, h, queries).start()

            if queries and there <= LAST[r]:

                @pl.when(me == there)
                def _():
                    recv[r, there] = send[r * n_head + h]

    project(0, KEYS)
    project(1, VALS)
    for r in RANK_ORDER[:2]:
        send_rank(r, False)
    project(2, QUER)
    extras()
    for r in RANK_ORDER[:2]:
        send_rank(r, True)
    for r in RANK_ORDER[2:]:
        send_rank(r, False)
        send_rank(r, True)
    loads[7].wait()

    def returned(r, h_here, j):
        return pltpu.make_async_remote_copy(
            src_ref=o_stage.at[r, j],
            dst_ref=a_buf.at[r, h_here],
            send_sem=o_send.at[r, j],
            recv_sem=o_recv.at[r, h_here],
            device_id={"kv": jnp.int32(j)},
            device_id_type=MESH,
        )

    def attend(r):
        shards = LAST[r] + 1
        span = shards * ROWS
        length = len_of[r]
        head = jnp.int32(0)
        for h in range(n_head):
            head = head + (me == PLACE[r][h]).astype(jnp.int32) * h

        pw_keys = jnp.concatenate([pw_ref[0].T] * (ROWS // L_CMP), axis=1)
        pw_vals = jnp.concatenate([pw_ref[1].T] * (ROWS // L_CMP), axis=1)
        weight[...] = jnp.concatenate([pw_keys, pw_vals], axis=0)
        lane_blk = iota((ROWS, ROWS), 0) // L_CMP
        lane_col = iota((ROWS, ROWS), 1)

        def prepare(j):
            @pl.when(me != j)
            def _():
                arrival(r, j, False).wait_recv()
                arrival(r, j, True).wait_recv()

            cols = slice(j * ROWS, (j + 1) * ROWS)
            q_ext[0:HD, cols] = recv[r, j, QUER:EXTRA, :]
            k_ext[0:HD, cols] = recv[r, j, KEYS:VALS, :]
            v_all[0:HD, cols] = recv[r, j, VALS:QUER, :]
            picks = recv[r, j, EXTRA:MSG, :].astype(F32)
            blocks = iota((32, ROWS), 0).astype(F32)
            hit = blocks == picks[8:9]
            for t in range(1, 8):
                hit = hit | (blocks == picks[8 + t : 9 + t])
            q_ext[HD : HD + 32, cols] = jnp.where(hit, 0.0, NEG).astype(BF)
            one_row = (iota((32, ROWS), 0) == 0).astype(F32)
            q_ext[HD + 32 :, cols] = one_row.astype(BF)
            key = j * ROWS + iota((32, ROWS), 1)
            k_ext[HD : HD + 32, cols] = (iota((32, ROWS), 0) == key // QB).astype(F32).astype(BF)
            k_ext[HD + 32 :, cols] = jnp.where(key >= length, one_row * NEG, 0.0).astype(BF)
            v_all[HD:, cols] = (iota((HD, ROWS), 0) == 0).astype(F32).astype(BF)
            prod = recv[r, j, KEYS:QUER, :].astype(F32) * weight[...]
            hi = prod.astype(BF)
            lo = (prod - hi.astype(F32)).astype(BF)
            group = jnp.where(lane_col == j * (ROWS // L_CMP) + lane_blk, 1.0, 0.0).astype(BF)
            return [hi, lo], [group, group]

        pool_sum[...] = jnp.zeros((2 * HD, ROWS), F32)
        for t in range(span // TILE):
            lo, hi = t * TILE, (t + 1) * TILE
            lefts, rights = [], []
            for i in range(TILE // ROWS):
                left_i, right_i = prepare(t * (TILE // ROWS) + i)
                lefts, rights = lefts + left_i, rights + right_i
            fresh = nn(jnp.concatenate(lefts, axis=1), jnp.concatenate(rights, axis=0))
            known = lane_col < t * (TILE // L_CMP)
            pool_sum[...] = jnp.where(known, pool_sum[...], fresh)
            pooled = pool_sum[...].astype(BF)
            key_pooled = jnp.concatenate([pooled[:HD], jnp.zeros((HD, ROWS), BF)], axis=0)
            val_pooled = pooled[HD:]
            q = q_ext[:, lo:hi].T
            scores = nn(q, k_ext[:, :hi])
            edge = jnp.where(
                iota((TILE, TILE), 1) <= iota((TILE, TILE), 0), scores[:, lo:hi], NEG
            )
            scores = edge if t == 0 else jnp.concatenate([scores[:, :lo], edge], axis=1)
            top = jnp.max(scores, axis=1, keepdims=True)
            e = jnp.exp(scores - top)
            summed = nt(e.astype(BF), v_all[:, :hi])
            picked_out = summed[:, :HD] / summed[:, HD : HD + 1]

            scores = nn(q, key_pooled)
            pos = lo + iota((TILE, ROWS), 0)
            end = iota((TILE, ROWS), 1) * L_CMP + (L_CMP - 1)
            usable = (end <= pos) & (end < length)
            top = jnp.max(jnp.where(usable, scores, NEG), axis=1, keepdims=True)
            e = jnp.where(usable, jnp.exp(jnp.where(usable, scores, NEG) - top), 0.0)
            tot = jnp.sum(e, axis=1, keepdims=True)
            pooled_out = nt(e.astype(BF), val_pooled) / jnp.where(tot > 0, tot, 1.0)

            both = jnp.concatenate([pooled_out, picked_out], axis=1).T
            for i in range(TILE // ROWS):
                j = t * (TILE // ROWS) + i
                g = recv[r, j, EXTRA:MSG, :].astype(F32)
                part = both[:, i * ROWS : (i + 1) * ROWS]
                mix = (g[0:1] + g[2:3]) * part[:HD] + (g[1:2] + g[3:4]) * part[HD:]
                alive = j * ROWS + iota((HD, ROWS), 1) < length
                o_stage[r, j] = jnp.where(alive, mix, 0.0).astype(BF)

                if j not in PAIRED:
                    before = RANK_ORDER[: RANK_ORDER.index(r)]
                    new = [
                        p
                        for p in PLACE[r]
                        if p < j and not any(p in PLACE[q] and j <= LAST[q] for q in before)
                    ]

                    @pl.when(any_of(me, new))
                    def _():
                        pl.semaphore_wait(ready_kv.at[j], 1)

                @pl.when(me != j)
                def _():
                    returned(r, head, j).start()

                @pl.when(me == j)
                def _():
                    a_buf[r, head] = o_stage[r, j]

    for r in RANK_ORDER:

        @pl.when(any_of(me, PLACE[r]))
        def _():
            attend(r)

    half = ROWS // 2
    lower, upper = pl.ds(0, half), pl.ds(half, half)

    def hop(r, block, rows, to, n):
        ref = x_buf.at[r, block] if rows is None else x_buf.at[r, block, rows]
        return pltpu.make_async_remote_copy(
            src_ref=ref,
            dst_ref=ref,
            send_sem=g_send.at[r, n],
            recv_sem=g_recv.at[r, n],
            device_id={"tp": to},
            device_id_type=MESH,
        )

    def sent(r, n):
        return hop(r, *(
            (tp, lower, right, 0),
            (tp, upper, right, 1),
            (tp, upper, left, 2),
            (tp, lower, left, 3),
            (left, lower, right, 4),
            (right, upper, left, 5),
            (tp, None, partner, 6),
            (left, None, partner, 7),
            (right, None, partner, 8),
            (far, None, partner, 9),
        )[n])

    def other(t):
        return t + 1 - 2 * lax.rem(t, 2)

    def received(r, n):
        return hop(r, *(
            (left, lower, left, 0),
            (left, upper, left, 1),
            (right, upper, right, 2),
            (right, lower, right, 3),
            (far, lower, left, 4),
            (far, upper, right, 5),
            (other(tp), None, partner, 6),
            (other(left), None, partner, 7),
            (other(right), None, partner, 8),
            (other(far), None, partner, 9),
        )[n])

    rows_each = ROWS // n_tp
    width = wo.shape[1]

    def column_copy(r, to):
        return pltpu.make_async_remote_copy(
            src_ref=y_buf.at[r, pl.ds(pl.multiple_of(to * rows_each, rows_each), rows_each)],
            dst_ref=o_buf.at[r, :, pl.ds(pl.multiple_of(tp * width, width), width)],
            send_sem=y_send.at[r, to],
            recv_sem=y_recv.at[r, tp],
            device_id={"tp": to},
            device_id_type=MESH,
        )

    def column_arrival(r, source):
        return pltpu.make_async_remote_copy(
            src_ref=y_buf.at[r, pl.ds(0, rows_each)],
            dst_ref=o_buf.at[r, :, pl.ds(pl.multiple_of(source * width, width), width)],
            send_sem=y_send.at[r, source],
            recv_sem=y_recv.at[r, source],
            device_id={"tp": source},
            device_id_type=MESH,
        )

    loads[8].wait()
    for t in range(n_tp):

        @pl.when(tp > t)
        def _():
            pl.semaphore_wait(ready_tp.at[t], 1)


    def own(r):
        for h in range(n_head):

            @pl.when(me != PLACE[r][h])
            def _():
                pltpu.make_async_remote_copy(
                    src_ref=o_stage.at[r, 0],
                    dst_ref=a_buf.at[r, h],
                    send_sem=o_send.at[r, 0],
                    recv_sem=o_recv.at[r, h],
                    device_id={"kv": jnp.int32(PLACE[r][h])},
                    device_id_type=MESH,
                ).wait_recv()

        x_buf[r, tp] = a_buf[r].reshape(n_head * HD, ROWS).T
        for n in (0, 2, 1, 3, 6):
            sent(r, n).start()

    def relay(r):
        received(r, 0).wait_recv()
        sent(r, 4).start()
        received(r, 2).wait_recv()
        sent(r, 5).start()
        received(r, 1).wait_recv()
        sent(r, 7).start()
        received(r, 3).wait_recv()
        sent(r, 8).start()

    def across(r):
        received(r, 4).wait_recv()
        received(r, 5).wait_recv()
        sent(r, 9).start()

    def mix(r):
        for n in (6, 7, 8, 9):
            received(r, n).wait_recv()
        rows = jnp.concatenate([x_buf[r, g] for g in range(n_tp)], axis=1)
        y_buf[r] = nn(rows, wo[...]).astype(BF)
        for step in range(1, n_tp):
            column_copy(r, lax.rem(tp + step, n_tp)).start()
        mine = pl.ds(pl.multiple_of(tp * rows_each, rows_each), rows_each)
        o_buf[r, :, pl.ds(pl.multiple_of(tp * width, width), width)] = y_buf[r, mine]

    def stage(step, r):
        @pl.when(me <= LAST[r])
        def _():
            step(r)

    first, second, third, last = RANK_ORDER
    for step, r in (
        (own, first), (own, second), (relay, first), (own, third), (relay, second),
        (across, first), (relay, third), (across, second), (mix, first), (across, third),
        (mix, second), (mix, third), (own, last), (relay, last), (across, last), (mix, last),
    ):
        stage(step, r)

    for r in range(n_seq):

        @pl.when(me > LAST[r])
        def _():
            o_buf[r] = jnp.zeros(o_buf.shape[1:], BF)

    for r in range(n_seq):

        @pl.when(me <= LAST[r])
        def _():
            for step in range(1, n_tp):
                column_arrival(r, lax.rem(tp + step, n_tp)).wait_recv()

    many = rows_each * n_seq
    want = iota((many, many), 0)
    have = iota((many, many), 1)
    pick = jnp.zeros((many, many), F32)
    for r in range(n_seq):
        hit = (have == r * rows_each + want // n_seq) & (lax.rem(want, n_seq) == seq_of[r])
        pick = jnp.where(hit, 1.0, pick)
    pick = pick.astype(BF)
    for c in range(n_tp):
        cols = slice(c * width, (c + 1) * width)
        rows = o_buf[:, :, cols].reshape(many, width)
        out_ref[:, :, cols] = nn(pick, rows).astype(BF).reshape(rows_each, n_seq, width)

    for r in range(n_seq):
        for h in range(n_head):

            @pl.when((me <= LAST[r]) & (me != PLACE[r][h]))
            def _():
                message(r, h, False).wait_send()
                message(r, h, True).wait_send()

        @pl.when(any_of(me, PLACE[r]))
        def _():
            for j in range(LAST[r] + 1):

                @pl.when(me != j)
                def _():
                    returned(r, 0, j).wait_send()

        @pl.when(me <= LAST[r])
        def _():
            for n in range(10):
                sent(r, n).wait_send()
            for step in range(1, n_tp):
                column_copy(r, lax.rem(tp + step, n_tp)).wait_send()


def body(tokens, lengths, chosen, w_query, w_key, w_value, w_gate, pool_weights, w_out):
    rows, n_seq, depth = tokens.shape
    n_head = w_query.shape[1] // HD
    n_kv, n_tp = lax.axis_size("kv"), lax.axis_size("tp")
    gate_rows = jnp.transpose(w_gate, (1, 2, 0))
    width = w_out.shape[1]
    total = rows * n_seq
    vmem = pl.BlockSpec(memory_space=pltpu.VMEM)
    hbm = pl.BlockSpec(memory_space=pl.ANY)
    dma = pltpu.SemaphoreType.DMA
    full = n_kv * rows

    def whole(*refs):
        kernel(n_kv, n_tp, n_seq, n_head, *refs)

    return pl.pallas_call(
        whole,
        out_shape=jax.ShapeDtypeStruct((rows // n_tp, n_seq, n_tp * width), BF),
        in_specs=[hbm] * 9,
        out_specs=vmem,
        scratch_shapes=[
            pltpu.VMEM((rows, n_seq, depth), BF),
            pltpu.VMEM((total, depth), BF),
            pltpu.VMEM((3, depth, n_head * HD), BF),
            pltpu.VMEM(gate_rows.shape, BF),
            pltpu.VMEM(pool_weights.shape, F32),
            pltpu.VMEM(w_out.shape, BF),
            pltpu.SMEM(lengths.shape, jnp.int32),
            pltpu.SMEM(chosen.shape, jnp.int32),
            pltpu.VMEM((total, total), BF),
            pltpu.VMEM((n_seq * n_head, MSG, rows), BF),
            pltpu.VMEM((n_seq, n_kv, MSG, rows), BF),
            pltpu.VMEM((128, full), BF),
            pltpu.VMEM((128, full), BF),
            pltpu.VMEM((128, full), BF),
            pltpu.VMEM((2 * HD, rows), F32),
            pltpu.VMEM((2 * HD, rows), F32),
            pltpu.VMEM((n_seq, n_kv, HD, rows), BF),
            pltpu.VMEM((n_seq, n_head, HD, rows), BF),
            pltpu.VMEM((n_seq, n_tp, rows, n_head * HD), BF),
            pltpu.VMEM((n_seq, rows, width), BF),
            pltpu.VMEM((n_seq, rows // n_tp, n_tp * width), BF),
            dma((9,)),
            dma((n_seq * n_head,)),
            dma((n_seq, n_kv)),
            dma((n_seq * n_head,)),
            dma((n_seq, n_kv)),
            dma((n_seq, n_kv)),
            dma((n_seq, n_head)),
            dma((n_seq, 10)),
            dma((n_seq, 10)),
            dma((n_seq, n_tp)),
            dma((n_seq, n_tp)),
            pltpu.SemaphoreType.REGULAR((n_kv,)),
            pltpu.SemaphoreType.REGULAR((n_tp,)),
        ],
        compiler_params=pltpu.CompilerParams(
            collective_id=0, has_side_effects=True, vmem_limit_bytes=60 * 2**20
        ),
    )(tokens, lengths, chosen, w_query, w_key, w_value, gate_rows, pool_weights, w_out)


def solution(mesh):
    placed = (
        P("kv", "grp", None),
        P("grp"),
        P("grp", "tp", "kv", None),
        P(None, "tp"),
        P(None, "tp"),
        P(None, "tp"),
        P(None, None, "tp"),
        P(),
        P(None, "tp"),
    )
    return jax.shard_map(
        body, mesh=mesh, in_specs=placed, out_specs=P(("kv", "tp"), "grp", None), check_vma=False
    )
```

```python
import jax
import jax.numpy as jnp
from jax import lax
from jax.experimental import pallas as pl
from jax.experimental.pallas import tpu as pltpu
from jax.sharding import PartitionSpec as P

HD = 64
QB = 64
L_CMP = 32
NEG = -1e30
BF = jnp.bfloat16
F32 = jnp.float32
MESH = pl.DeviceIdType.MESH

ROWS = 128
AUX = 16
MSG = 3 * HD + AUX
KEYS, VALS, QUER, EXTRA = 0, HD, 2 * HD, 3 * HD
LAST = (15, 11, 7, 5)
PLACE = (
    (9, 11, 12, 13),
    (4, 5, 6, 7),
    (3, 4, 1, 2),
    (2, 3, 1, 5),
)
RANK_ORDER = (3, 2, 1, 0)
TILE = 256
SHARDS = LAST[0] + 1
PAIRED = sorted({p for places in PLACE for p in places})


def returns_to(i, j):
    return any(i in PLACE[r] and j <= LAST[r] for r in range(len(PLACE)))


def sends_to(i, j):
    asked = any(j in PLACE[r] and i <= LAST[r] for r in range(len(PLACE)))
    return asked or returns_to(i, j)


def any_of(me, places):
    here = me < 0
    for p in places:
        here = here | (me == p)
    return here


def iota(shape, dim):
    return lax.broadcasted_iota(jnp.int32, shape, dim)


def nt(a, b):
    return lax.dot_general(a, b, (((1,), (1,)), ((), ())), preferred_element_type=F32)


def nn(a, b):
    return jnp.dot(a, b, preferred_element_type=F32)


def kernel(
    n_kv, n_tp, n_seq, n_head,
    tok_hbm, len_hbm, chosen_hbm, wq_hbm, wk_hbm, wv_hbm, wg_hbm, pw_hbm, wo_hbm,
    out_ref,
    tok, flat, w_buf, wg, pw_ref, wo, len_ref, chosen_ref,
    sel_t, send, recv, k_ext, q_ext, v_all, weight, pool_sum, o_stage, a_buf, x_buf, y_buf, o_buf,
    load_sem, q_send, q_recv, o_send, o_recv, g_send, g_recv, y_send, y_recv,
    ready_kv, ready_tp,
):
    me = lax.axis_index("kv")
    tp = lax.axis_index("tp")
    chips = n_tp // 2
    core = lax.rem(tp, 2)
    chip = tp // 2
    right = lax.rem(chip + 1, chips) * 2 + core
    left = lax.rem(chip + chips - 1, chips) * 2 + core
    far = lax.rem(chip + 2, chips) * 2 + core
    partner = chip * 2 + 1 - core

    barrier = pltpu.get_barrier_semaphore()
    for j in range(n_kv):

        @pl.when(me < j)
        def _():
            pl.semaphore_signal(
                barrier, inc=1, device_id={"kv": jnp.int32(j)}, device_id_type=MESH
            )

    for t in range(n_tp):

        @pl.when(tp > t)
        def _():
            pl.semaphore_signal(
                barrier, inc=1, device_id={"tp": jnp.int32(t)}, device_id_type=MESH
            )

    loads = [
        pltpu.make_async_copy(len_hbm, len_ref, load_sem.at[0]),
        pltpu.make_async_copy(tok_hbm, tok, load_sem.at[1]),
        pltpu.make_async_copy(wk_hbm, w_buf.at[0], load_sem.at[2]),
        pltpu.make_async_copy(wv_hbm, w_buf.at[1], load_sem.at[3]),
        pltpu.make_async_copy(wq_hbm, w_buf.at[2], load_sem.at[4]),
        pltpu.make_async_copy(wg_hbm, wg, load_sem.at[5]),
        pltpu.make_async_copy(chosen_hbm, chosen_ref, load_sem.at[6]),
        pltpu.make_async_copy(pw_hbm, pw_ref, load_sem.at[7]),
        pltpu.make_async_copy(wo_hbm, wo, load_sem.at[8]),
    ]
    for copy in loads:
        copy.start()
    told = me + n_tp - 1 - tp

    @pl.when(told > 0)
    def _():
        pl.semaphore_wait(barrier, told)

    for i in range(n_kv):
        later = [j for j in range(i + 1, n_kv) if sends_to(i, j)]

        @pl.when(any_of(me, later))
        def _():
            pl.semaphore_signal(
                ready_kv.at[me], inc=1, device_id={"kv": jnp.int32(i)}, device_id_type=MESH
            )

    for t in range(n_tp):

        @pl.when(tp < t)
        def _():
            pl.semaphore_signal(
                ready_tp.at[tp], inc=1, device_id={"tp": jnp.int32(t)}, device_id_type=MESH
            )

    loads[0].wait()

    lens = [len_ref[s] for s in range(n_seq)]
    ranks = []
    for s in range(n_seq):
        rank = jnp.int32(0)
        for o in range(n_seq):
            if o != s:
                ahead = (lens[o] >= lens[s]) if o < s else (lens[o] > lens[s])
                rank = rank + ahead.astype(jnp.int32)
        ranks.append(rank)
    seq_of, len_of = [], []
    for r in range(n_seq):
        seq, length = jnp.int32(0), jnp.int32(0)
        for s in range(n_seq):
            hit = (ranks[s] == r).astype(jnp.int32)
            seq = seq + hit * s
            length = length + hit * lens[s]
        seq_of.append(seq)
        len_of.append(length)

    total = ROWS * n_seq
    row = iota((total, ROWS), 0)
    col = iota((total, ROWS), 1)
    for r in range(n_seq):
        hit = row == col * n_seq + seq_of[r]
        sel_t[:, r * ROWS : (r + 1) * ROWS] = jnp.where(hit, 1.0, 0.0).astype(BF)

    loads[1].wait()
    flat[...] = tok[...].reshape(flat.shape)

    def project(slot, base):
        loads[2 + slot].wait()
        made = nn(flat[...], w_buf[slot]).astype(BF).T
        placed = nn(made, sel_t[...])
        if base == QUER:
            placed = placed * HD**-0.5
        placed = placed.astype(BF)
        for r in range(n_seq):
            for h in range(n_head):
                send[r * n_head + h, base : base + HD, :] = placed[
                    h * HD : (h + 1) * HD, r * ROWS : (r + 1) * ROWS
                ]

    def extras():
        loads[5].wait()
        loads[6].wait()
        gates = jax.nn.sigmoid(nt(wg[...].reshape(2 * n_head, wg.shape[2]), flat[...]))
        gate_hi = gates.astype(BF)
        gate_lo = (gates - gate_hi.astype(F32)).astype(BF)
        gate_rows = nn(jnp.concatenate([gate_hi, gate_lo], axis=0), sel_t[...])
        n_blk, top = chosen_ref.shape[2:]
        slot = iota((top, ROWS), 0)
        blk = iota((top, ROWS), 1) // (ROWS // n_blk)
        for r in range(n_seq):
            cols = slice(r * ROWS, (r + 1) * ROWS)
            for h in range(n_head):
                picked = jnp.zeros((top, ROWS), jnp.int32)
                for b in range(n_blk):
                    for t in range(top):
                        at = (slot == t) & (blk == b)
                        picked = jnp.where(at, chosen_ref[seq_of[r], h, b, t], picked)
                kinds = [
                    gate_rows[g * n_head + h : g * n_head + h + 1, cols] for g in range(4)
                ]
                rest = jnp.zeros((AUX - top - 4, ROWS), F32)
                aux = jnp.concatenate([*kinds, rest, picked.astype(F32)], axis=0)
                send[r * n_head + h, EXTRA:, :] = aux.astype(BF)

    wholes = ((0, MSG),)
    halves = ((0, QUER), (QUER, MSG - QUER))
    thirds = ((KEYS, HD), (VALS, HD), (QUER, MSG - QUER))
    parts_of = {3: thirds, 2: thirds, 1: halves, 0: wholes}

    def message(r, h, part):
        rows = pl.ds(*parts_of[r][part])
        return pltpu.make_async_remote_copy(
            src_ref=send.at[r * n_head + h, rows],
            dst_ref=recv.at[r, me, rows],
            send_sem=q_send.at[part, r * n_head + h],
            recv_sem=q_recv.at[part, r, me],
            device_id={"kv": jnp.int32(PLACE[r][h])},
            device_id_type=MESH,
        )

    def arrival(r, j, part):
        rows = pl.ds(*parts_of[r][part])
        return pltpu.make_async_remote_copy(
            src_ref=send.at[0, rows],
            dst_ref=recv.at[r, j, rows],
            send_sem=q_send.at[part, 0],
            recv_sem=q_recv.at[part, r, j],
            device_id={"kv": jnp.int32(0)},
            device_id_type=MESH,
        )

    asked = set()

    def send_rank(r, part):
        for h in sorted(range(n_head), key=lambda h: PLACE[r][h]):
            there = PLACE[r][h]
            if there not in asked:
                asked.add(there)

                @pl.when(any_of(me, [i for i in range(there) if sends_to(i, there)]))
                def _():
                    pl.semaphore_wait(ready_kv.at[there], 1)

            @pl.when((me <= LAST[r]) & (me != there))
            def _():
                message(r, h, part).start()

            if part == len(parts_of[r]) - 1 and there <= LAST[r]:

                @pl.when(me == there)
                def _():
                    recv[r, there] = send[r * n_head + h]

    project(0, KEYS)
    send_rank(3, 0)
    send_rank(2, 0)
    project(1, VALS)
    send_rank(3, 1)
    send_rank(2, 1)
    project(2, QUER)
    send_rank(1, 0)
    extras()
    send_rank(3, 2)
    send_rank(2, 2)
    send_rank(1, 1)
    send_rank(0, 0)
    loads[7].wait()

    def returned(r, h_here, j):
        return pltpu.make_async_remote_copy(
            src_ref=o_stage.at[r, j],
            dst_ref=a_buf.at[r, h_here],
            send_sem=o_send.at[r, j],
            recv_sem=o_recv.at[r, h_here],
            device_id={"kv": jnp.int32(j)},
            device_id_type=MESH,
        )

    def attend(r):
        shards = LAST[r] + 1
        span = shards * ROWS
        length = len_of[r]
        head = jnp.int32(0)
        for h in range(n_head):
            head = head + (me == PLACE[r][h]).astype(jnp.int32) * h

        pw_keys = jnp.concatenate([pw_ref[0].T] * (ROWS // L_CMP), axis=1)
        pw_vals = jnp.concatenate([pw_ref[1].T] * (ROWS // L_CMP), axis=1)
        weight[...] = jnp.concatenate([pw_keys, pw_vals], axis=0)
        lane_blk = iota((ROWS, ROWS), 0) // L_CMP
        lane_col = iota((ROWS, ROWS), 1)

        def prepare(j):
            @pl.when(me != j)
            def _():
                for part in range(len(parts_of[r])):
                    arrival(r, j, part).wait_recv()

            cols = slice(j * ROWS, (j + 1) * ROWS)
            q_ext[0:HD, cols] = recv[r, j, QUER:EXTRA, :]
            k_ext[0:HD, cols] = recv[r, j, KEYS:VALS, :]
            v_all[0:HD, cols] = recv[r, j, VALS:QUER, :]
            picks = recv[r, j, EXTRA:MSG, :].astype(F32)
            blocks = iota((32, ROWS), 0).astype(F32)
            hit = blocks == picks[8:9]
            for t in range(1, 8):
                hit = hit | (blocks == picks[8 + t : 9 + t])
            q_ext[HD : HD + 32, cols] = jnp.where(hit, 0.0, NEG).astype(BF)
            one_row = (iota((32, ROWS), 0) == 0).astype(F32)
            q_ext[HD + 32 :, cols] = one_row.astype(BF)
            key = j * ROWS + iota((32, ROWS), 1)
            k_ext[HD : HD + 32, cols] = (iota((32, ROWS), 0) == key // QB).astype(F32).astype(BF)
            k_ext[HD + 32 :, cols] = jnp.where(key >= length, one_row * NEG, 0.0).astype(BF)
            v_all[HD:, cols] = (iota((HD, ROWS), 0) == 0).astype(F32).astype(BF)
            prod = recv[r, j, KEYS:QUER, :].astype(F32) * weight[...]
            hi = prod.astype(BF)
            lo = (prod - hi.astype(F32)).astype(BF)
            group = jnp.where(lane_col == j * (ROWS // L_CMP) + lane_blk, 1.0, 0.0).astype(BF)
            return [hi, lo], [group, group]

        pool_sum[...] = jnp.zeros((2 * HD, ROWS), F32)
        for t in range(span // TILE):
            lo, hi = t * TILE, (t + 1) * TILE
            lefts, rights = [], []
            for i in range(TILE // ROWS):
                left_i, right_i = prepare(t * (TILE // ROWS) + i)
                lefts, rights = lefts + left_i, rights + right_i
            fresh = nn(jnp.concatenate(lefts, axis=1), jnp.concatenate(rights, axis=0))
            known = lane_col < t * (TILE // L_CMP)
            pool_sum[...] = jnp.where(known, pool_sum[...], fresh)
            pooled = pool_sum[...].astype(BF)
            key_pooled = jnp.concatenate([pooled[:HD], jnp.zeros((HD, ROWS), BF)], axis=0)
            val_pooled = pooled[HD:]
            q = q_ext[:, lo:hi].T
            scores = nn(q, k_ext[:, :hi])
            edge = jnp.where(
                iota((TILE, TILE), 1) <= iota((TILE, TILE), 0), scores[:, lo:hi], NEG
            )
            scores = edge if t == 0 else jnp.concatenate([scores[:, :lo], edge], axis=1)
            top = jnp.max(scores, axis=1, keepdims=True)
            e = jnp.exp(scores - top)
            summed = nt(e.astype(BF), v_all[:, :hi])
            picked_out = summed[:, :HD] / summed[:, HD : HD + 1]

            scores = nn(q, key_pooled)
            pos = lo + iota((TILE, ROWS), 0)
            end = iota((TILE, ROWS), 1) * L_CMP + (L_CMP - 1)
            usable = (end <= pos) & (end < length)
            top = jnp.max(jnp.where(usable, scores, NEG), axis=1, keepdims=True)
            e = jnp.where(usable, jnp.exp(jnp.where(usable, scores, NEG) - top), 0.0)
            tot = jnp.sum(e, axis=1, keepdims=True)
            pooled_out = nt(e.astype(BF), val_pooled) / jnp.where(tot > 0, tot, 1.0)

            both = jnp.concatenate([pooled_out, picked_out], axis=1).T
            for i in range(TILE // ROWS):
                j = t * (TILE // ROWS) + i
                g = recv[r, j, EXTRA:MSG, :].astype(F32)
                part = both[:, i * ROWS : (i + 1) * ROWS]
                mix = (g[0:1] + g[2:3]) * part[:HD] + (g[1:2] + g[3:4]) * part[HD:]
                alive = j * ROWS + iota((HD, ROWS), 1) < length
                o_stage[r, j] = jnp.where(alive, mix, 0.0).astype(BF)

                if j not in PAIRED:
                    before = RANK_ORDER[: RANK_ORDER.index(r)]
                    new = [
                        p
                        for p in PLACE[r]
                        if p < j and not any(p in PLACE[q] and j <= LAST[q] for q in before)
                    ]

                    @pl.when(any_of(me, new))
                    def _():
                        pl.semaphore_wait(ready_kv.at[j], 1)

                @pl.when(me != j)
                def _():
                    returned(r, head, j).start()

                @pl.when(me == j)
                def _():
                    a_buf[r, head] = o_stage[r, j]

    for r in RANK_ORDER:

        @pl.when(any_of(me, PLACE[r]))
        def _():
            attend(r)

    half = ROWS // 2
    lower, upper = pl.ds(0, half), pl.ds(half, half)

    def hop(r, block, rows, to, n):
        ref = x_buf.at[r, block] if rows is None else x_buf.at[r, block, rows]
        return pltpu.make_async_remote_copy(
            src_ref=ref,
            dst_ref=ref,
            send_sem=g_send.at[r, n],
            recv_sem=g_recv.at[r, n],
            device_id={"tp": to},
            device_id_type=MESH,
        )

    def sent(r, n):
        return hop(r, *(
            (tp, lower, right, 0),
            (tp, upper, right, 1),
            (tp, upper, left, 2),
            (tp, lower, left, 3),
            (left, lower, right, 4),
            (right, upper, left, 5),
            (tp, None, partner, 6),
            (left, None, partner, 7),
            (right, None, partner, 8),
            (far, None, partner, 9),
        )[n])

    def other(t):
        return t + 1 - 2 * lax.rem(t, 2)

    def received(r, n):
        return hop(r, *(
            (left, lower, left, 0),
            (left, upper, left, 1),
            (right, upper, right, 2),
            (right, lower, right, 3),
            (far, lower, left, 4),
            (far, upper, right, 5),
            (other(tp), None, partner, 6),
            (other(left), None, partner, 7),
            (other(right), None, partner, 8),
            (other(far), None, partner, 9),
        )[n])

    rows_each = ROWS // n_tp
    width = wo.shape[1]

    def column_copy(r, to):
        return pltpu.make_async_remote_copy(
            src_ref=y_buf.at[r, pl.ds(pl.multiple_of(to * rows_each, rows_each), rows_each)],
            dst_ref=o_buf.at[r, :, pl.ds(pl.multiple_of(tp * width, width), width)],
            send_sem=y_send.at[r, to],
            recv_sem=y_recv.at[r, tp],
            device_id={"tp": to},
            device_id_type=MESH,
        )

    def column_arrival(r, source):
        return pltpu.make_async_remote_copy(
            src_ref=y_buf.at[r, pl.ds(0, rows_each)],
            dst_ref=o_buf.at[r, :, pl.ds(pl.multiple_of(source * width, width), width)],
            send_sem=y_send.at[r, source],
            recv_sem=y_recv.at[r, source],
            device_id={"tp": source},
            device_id_type=MESH,
        )

    loads[8].wait()
    for t in range(n_tp):

        @pl.when(tp > t)
        def _():
            pl.semaphore_wait(ready_tp.at[t], 1)


    def own(r):
        for h in range(n_head):

            @pl.when(me != PLACE[r][h])
            def _():
                pltpu.make_async_remote_copy(
                    src_ref=o_stage.at[r, 0],
                    dst_ref=a_buf.at[r, h],
                    send_sem=o_send.at[r, 0],
                    recv_sem=o_recv.at[r, h],
                    device_id={"kv": jnp.int32(PLACE[r][h])},
                    device_id_type=MESH,
                ).wait_recv()

        x_buf[r, tp] = a_buf[r].reshape(n_head * HD, ROWS).T
        for n in (0, 2, 1, 3, 6):
            sent(r, n).start()

    def relay(r):
        received(r, 0).wait_recv()
        sent(r, 4).start()
        received(r, 2).wait_recv()
        sent(r, 5).start()
        received(r, 1).wait_recv()
        sent(r, 7).start()
        received(r, 3).wait_recv()
        sent(r, 8).start()

    def across(r):
        received(r, 4).wait_recv()
        received(r, 5).wait_recv()
        sent(r, 9).start()

    def mix(r):
        for n in (6, 7, 8, 9):
            received(r, n).wait_recv()
        rows = jnp.concatenate([x_buf[r, g] for g in range(n_tp)], axis=1)
        y_buf[r] = nn(rows, wo[...]).astype(BF)
        for step in range(1, n_tp):
            column_copy(r, lax.rem(tp + step, n_tp)).start()
        mine = pl.ds(pl.multiple_of(tp * rows_each, rows_each), rows_each)
        o_buf[r, :, pl.ds(pl.multiple_of(tp * width, width), width)] = y_buf[r, mine]

    def stage(step, r):
        @pl.when(me <= LAST[r])
        def _():
            step(r)

    first, second, third, last = RANK_ORDER
    for step, r in (
        (own, first), (own, second), (relay, first), (own, third), (relay, second), (own, last),
        (across, first), (relay, third), (across, second), (mix, first), (relay, last),
        (across, third), (mix, second), (across, last), (mix, third), (mix, last),
    ):
        stage(step, r)

    for r in range(n_seq):

        @pl.when(me > LAST[r])
        def _():
            o_buf[r] = jnp.zeros(o_buf.shape[1:], BF)

    for r in range(n_seq):

        @pl.when(me <= LAST[r])
        def _():
            for step in range(1, n_tp):
                column_arrival(r, lax.rem(tp + step, n_tp)).wait_recv()

    many = rows_each * n_seq
    want = iota((many, many), 0)
    have = iota((many, many), 1)
    pick = jnp.zeros((many, many), F32)
    for r in range(n_seq):
        hit = (have == r * rows_each + want // n_seq) & (lax.rem(want, n_seq) == seq_of[r])
        pick = jnp.where(hit, 1.0, pick)
    pick = pick.astype(BF)
    for c in range(n_tp):
        cols = slice(c * width, (c + 1) * width)
        rows = o_buf[:, :, cols].reshape(many, width)
        out_ref[:, :, cols] = nn(pick, rows).astype(BF).reshape(rows_each, n_seq, width)

    for r in range(n_seq):
        for h in range(n_head):

            @pl.when((me <= LAST[r]) & (me != PLACE[r][h]))
            def _():
                for part in range(len(parts_of[r])):
                    message(r, h, part).wait_send()

        @pl.when(any_of(me, PLACE[r]))
        def _():
            for j in range(LAST[r] + 1):

                @pl.when(me != j)
                def _():
                    returned(r, 0, j).wait_send()

        @pl.when(me <= LAST[r])
        def _():
            for n in range(10):
                sent(r, n).wait_send()
            for step in range(1, n_tp):
                column_copy(r, lax.rem(tp + step, n_tp)).wait_send()


def body(tokens, lengths, chosen, w_query, w_key, w_value, w_gate, pool_weights, w_out):
    rows, n_seq, depth = tokens.shape
    n_head = w_query.shape[1] // HD
    n_kv, n_tp = lax.axis_size("kv"), lax.axis_size("tp")
    gate_rows = jnp.transpose(w_gate, (1, 2, 0))
    width = w_out.shape[1]
    total = rows * n_seq
    vmem = pl.BlockSpec(memory_space=pltpu.VMEM)
    hbm = pl.BlockSpec(memory_space=pl.ANY)
    dma = pltpu.SemaphoreType.DMA
    full = n_kv * rows

    def whole(*refs):
        kernel(n_kv, n_tp, n_seq, n_head, *refs)

    return pl.pallas_call(
        whole,
        out_shape=jax.ShapeDtypeStruct((rows // n_tp, n_seq, n_tp * width), BF),
        in_specs=[hbm] * 9,
        out_specs=vmem,
        scratch_shapes=[
            pltpu.VMEM((rows, n_seq, depth), BF),
            pltpu.VMEM((total, depth), BF),
            pltpu.VMEM((3, depth, n_head * HD), BF),
            pltpu.VMEM(gate_rows.shape, BF),
            pltpu.VMEM(pool_weights.shape, F32),
            pltpu.VMEM(w_out.shape, BF),
            pltpu.SMEM(lengths.shape, jnp.int32),
            pltpu.SMEM(chosen.shape, jnp.int32),
            pltpu.VMEM((total, total), BF),
            pltpu.VMEM((n_seq * n_head, MSG, rows), BF),
            pltpu.VMEM((n_seq, n_kv, MSG, rows), BF),
            pltpu.VMEM((128, full), BF),
            pltpu.VMEM((128, full), BF),
            pltpu.VMEM((128, full), BF),
            pltpu.VMEM((2 * HD, rows), F32),
            pltpu.VMEM((2 * HD, rows), F32),
            pltpu.VMEM((n_seq, n_kv, HD, rows), BF),
            pltpu.VMEM((n_seq, n_head, HD, rows), BF),
            pltpu.VMEM((n_seq, n_tp, rows, n_head * HD), BF),
            pltpu.VMEM((n_seq, rows, width), BF),
            pltpu.VMEM((n_seq, rows // n_tp, n_tp * width), BF),
            dma((9,)),
            dma((3, n_seq * n_head)),
            dma((3, n_seq, n_kv)),
            dma((n_seq, n_kv)),
            dma((n_seq, n_head)),
            dma((n_seq, 10)),
            dma((n_seq, 10)),
            dma((n_seq, n_tp)),
            dma((n_seq, n_tp)),
            pltpu.SemaphoreType.REGULAR((n_kv,)),
            pltpu.SemaphoreType.REGULAR((n_tp,)),
        ],
        compiler_params=pltpu.CompilerParams(
            collective_id=0, has_side_effects=True, vmem_limit_bytes=60 * 2**20
        ),
    )(tokens, lengths, chosen, w_query, w_key, w_value, gate_rows, pool_weights, w_out)


def solution(mesh):
    placed = (
        P("kv", "grp", None),
        P("grp"),
        P("grp", "tp", "kv", None),
        P(None, "tp"),
        P(None, "tp"),
        P(None, "tp"),
        P(None, None, "tp"),
        P(),
        P(None, "tp"),
    )
    return jax.shard_map(
        body, mesh=mesh, in_specs=placed, out_specs=P(("kv", "tp"), "grp", None), check_vma=False
    )
```

```python
import jax
import jax.numpy as jnp
from jax import lax
from jax.experimental import pallas as pl
from jax.experimental.pallas import tpu as pltpu
from jax.sharding import PartitionSpec as P

HD = 64
QB = 64
L_CMP = 32
NEG = -1e30
BF = jnp.bfloat16
F32 = jnp.float32
MESH = pl.DeviceIdType.MESH

ROWS = 128
AUX = 16
MSG = 3 * HD + AUX
KEYS, VALS, QUER, EXTRA = 0, HD, 2 * HD, 3 * HD
LAST = (15, 11, 7, 5)
PLACE = (
    (9, 11, 12, 13),
    (4, 5, 6, 7),
    (3, 4, 1, 2),
    (2, 3, 1, 5),
)
RANK_ORDER = (3, 2, 1, 0)
TILE = 256
AHEAD = 2
RELAY_SEM = (0, 1, 2, 3, 4, 4, 5, 5, 5, 5)
SHARDS = LAST[0] + 1
PAIRED = sorted({p for places in PLACE for p in places})


def returns_to(i, j):
    return any(i in PLACE[r] and j <= LAST[r] for r in range(len(PLACE)))


def sends_to(i, j):
    asked = any(j in PLACE[r] and i <= LAST[r] for r in range(len(PLACE)))
    return asked or returns_to(i, j)


FIRST = [sum(LAST[:r]) + r for r in range(len(LAST))]


def any_of(me, places):
    here = me < 0
    for p in places:
        here = here | (me == p)
    return here


def iota(shape, dim):
    return lax.broadcasted_iota(jnp.int32, shape, dim)


def nt(a, b):
    return lax.dot_general(a, b, (((1,), (1,)), ((), ())), preferred_element_type=F32)


def nn(a, b):
    return jnp.dot(a, b, preferred_element_type=F32)


def kernel(
    n_kv, n_tp, n_seq, n_head,
    tok_hbm, len_hbm, chosen_hbm, wq_hbm, wk_hbm, wv_hbm, wg_hbm, pw_hbm, wo_hbm,
    out_ref,
    tok, flat, w_buf, wg, pw_ref, wo, len_ref, chosen_ref,
    sel_t, send, recv, k_ext, q_ext, v_all, weight, pool_sum, o_stage, a_buf, x_buf, y_buf, o_buf,
    load_sem, q_send, q_recv, o_send, o_recv, g_send, g_recv, y_send, y_recv,
    ready_kv, ready_tp,
):
    me = lax.axis_index("kv")
    tp = lax.axis_index("tp")
    chips = n_tp // 2
    core = lax.rem(tp, 2)
    chip = tp // 2
    right = lax.rem(chip + 1, chips) * 2 + core
    left = lax.rem(chip + chips - 1, chips) * 2 + core
    far = lax.rem(chip + 2, chips) * 2 + core
    partner = chip * 2 + 1 - core

    barrier = pltpu.get_barrier_semaphore()
    for j in range(n_kv):

        @pl.when(me < j)
        def _():
            pl.semaphore_signal(
                barrier, inc=1, device_id={"kv": jnp.int32(j)}, device_id_type=MESH
            )

    for t in range(n_tp):

        @pl.when(tp > t)
        def _():
            pl.semaphore_signal(
                barrier, inc=1, device_id={"tp": jnp.int32(t)}, device_id_type=MESH
            )

    loads = [
        pltpu.make_async_copy(len_hbm, len_ref, load_sem.at[0]),
        pltpu.make_async_copy(tok_hbm, tok, load_sem.at[1]),
        pltpu.make_async_copy(wk_hbm, w_buf.at[0], load_sem.at[2]),
        pltpu.make_async_copy(wv_hbm, w_buf.at[1], load_sem.at[3]),
        pltpu.make_async_copy(wq_hbm, w_buf.at[2], load_sem.at[4]),
        pltpu.make_async_copy(wg_hbm, wg, load_sem.at[5]),
        pltpu.make_async_copy(chosen_hbm, chosen_ref, load_sem.at[6]),
        pltpu.make_async_copy(pw_hbm, pw_ref, load_sem.at[7]),
        pltpu.make_async_copy(wo_hbm, wo, load_sem.at[8]),
    ]
    for copy in loads:
        copy.start()
    told = me + n_tp - 1 - tp

    @pl.when(told > 0)
    def _():
        pl.semaphore_wait(barrier, told)

    for i in range(n_kv):
        later = [j for j in range(i + 1, n_kv) if sends_to(i, j)]

        @pl.when(any_of(me, later))
        def _():
            pl.semaphore_signal(
                ready_kv.at[me], inc=1, device_id={"kv": jnp.int32(i)}, device_id_type=MESH
            )

    for t in range(n_tp):

        @pl.when(tp < t)
        def _():
            pl.semaphore_signal(
                ready_tp.at[tp], inc=1, device_id={"tp": jnp.int32(t)}, device_id_type=MESH
            )

    loads[0].wait()

    lens = [len_ref[s] for s in range(n_seq)]
    ranks = []
    for s in range(n_seq):
        rank = jnp.int32(0)
        for o in range(n_seq):
            if o != s:
                ahead = (lens[o] >= lens[s]) if o < s else (lens[o] > lens[s])
                rank = rank + ahead.astype(jnp.int32)
        ranks.append(rank)
    seq_of, len_of = [], []
    for r in range(n_seq):
        seq, length = jnp.int32(0), jnp.int32(0)
        for s in range(n_seq):
            hit = (ranks[s] == r).astype(jnp.int32)
            seq = seq + hit * s
            length = length + hit * lens[s]
        seq_of.append(seq)
        len_of.append(length)

    total = ROWS * n_seq
    row = iota((total, ROWS), 0)
    col = iota((total, ROWS), 1)
    for r in range(n_seq):
        hit = row == col * n_seq + seq_of[r]
        sel_t[:, r * ROWS : (r + 1) * ROWS] = jnp.where(hit, 1.0, 0.0).astype(BF)

    loads[1].wait()
    flat[...] = tok[...].reshape(flat.shape)

    def project(slot, base):
        loads[2 + slot].wait()
        made = nn(flat[...], w_buf[slot]).astype(BF).T
        placed = nn(made, sel_t[...])
        if base == QUER:
            placed = placed * HD**-0.5
        placed = placed.astype(BF)
        for r in range(n_seq):
            for h in range(n_head):
                send[r * n_head + h, base : base + HD, :] = placed[
                    h * HD : (h + 1) * HD, r * ROWS : (r + 1) * ROWS
                ]

    def extras():
        loads[5].wait()
        loads[6].wait()
        gates = jax.nn.sigmoid(nt(wg[...].reshape(2 * n_head, wg.shape[2]), flat[...]))
        gate_hi = gates.astype(BF)
        gate_lo = (gates - gate_hi.astype(F32)).astype(BF)
        gate_rows = nn(jnp.concatenate([gate_hi, gate_lo], axis=0), sel_t[...])
        n_blk, top = chosen_ref.shape[2:]
        slot = iota((top, ROWS), 0)
        blk = iota((top, ROWS), 1) // (ROWS // n_blk)
        for r in range(n_seq):
            cols = slice(r * ROWS, (r + 1) * ROWS)
            for h in range(n_head):
                picked = jnp.zeros((top, ROWS), jnp.int32)
                for b in range(n_blk):
                    for t in range(top):
                        at = (slot == t) & (blk == b)
                        picked = jnp.where(at, chosen_ref[seq_of[r], h, b, t], picked)
                kinds = [
                    gate_rows[g * n_head + h : g * n_head + h + 1, cols] for g in range(4)
                ]
                rest = jnp.zeros((AUX - top - 4, ROWS), F32)
                aux = jnp.concatenate([*kinds, rest, picked.astype(F32)], axis=0)
                send[r * n_head + h, EXTRA:, :] = aux.astype(BF)

    wholes = ((0, MSG),)
    halves = ((0, QUER), (QUER, MSG - QUER))
    thirds = ((KEYS, HD), (VALS, HD), (QUER, MSG - QUER))
    parts_of = {3: thirds, 2: thirds, 1: halves, 0: wholes}

    def message(r, h, part):
        rows = pl.ds(*parts_of[r][part])
        return pltpu.make_async_remote_copy(
            src_ref=send.at[r * n_head + h, rows],
            dst_ref=recv.at[r, me, rows],
            send_sem=q_send.at[r],
            recv_sem=q_recv.at[FIRST[r] + me],
            device_id={"kv": jnp.int32(PLACE[r][h])},
            device_id_type=MESH,
        )

    def arrival(r, j):
        return pltpu.make_async_remote_copy(
            src_ref=send.at[0],
            dst_ref=recv.at[r, j],
            send_sem=q_send.at[r],
            recv_sem=q_recv.at[FIRST[r] + j],
            device_id={"kv": jnp.int32(0)},
            device_id_type=MESH,
        )

    def departures(r, count):
        return pltpu.make_async_remote_copy(
            src_ref=send.at[pl.ds(0, count)],
            dst_ref=send.at[pl.ds(0, count)],
            send_sem=q_send.at[r],
            recv_sem=q_recv.at[0],
            device_id={"kv": jnp.int32(0)},
            device_id_type=MESH,
        )

    def await_ready(there):
        @pl.when(any_of(me, [i for i in range(there) if sends_to(i, there)]))
        def _():
            pl.semaphore_wait(ready_kv.at[there], 1)

    asked = set()

    def send_rank(r, part):
        for h in sorted(range(n_head), key=lambda h: PLACE[r][h]):
            there = PLACE[r][h]
            if there not in asked:
                asked.add(there)
                await_ready(there)

            @pl.when((me <= LAST[r]) & (me != there))
            def _():
                message(r, h, part).start()

    ahead = me < AHEAD
    project(0, KEYS)

    @pl.when(jnp.logical_not(ahead))
    def _():
        send_rank(3, 0)
        send_rank(2, 0)

    project(1, VALS)

    @pl.when(jnp.logical_not(ahead))
    def _():
        send_rank(3, 1)
        send_rank(2, 1)

    project(2, QUER)

    @pl.when(jnp.logical_not(ahead))
    def _():
        send_rank(1, 0)

    extras()
    for r in range(n_seq):
        for h in range(n_head):
            there = PLACE[r][h]
            if there <= LAST[r]:

                @pl.when(me == there)
                def _():
                    recv[r, there] = send[r * n_head + h]

    @pl.when(ahead)
    def _():
        for there in PAIRED:
            await_ready(there)
            for r in (3, 2, 1, 0):
                for h in range(n_head):
                    if PLACE[r][h] == there:
                        for part in range(len(parts_of[r])):

                            @pl.when(me != there)
                            def _():
                                message(r, h, part).start()

    @pl.when(jnp.logical_not(ahead))
    def _():
        send_rank(3, 2)
        send_rank(2, 2)
        send_rank(1, 1)
        send_rank(0, 0)

    loads[7].wait()

    def returned(r, h_here, j):
        return pltpu.make_async_remote_copy(
            src_ref=o_stage.at[r, j],
            dst_ref=a_buf.at[r, h_here],
            send_sem=o_send.at[r],
            recv_sem=o_recv.at[r],
            device_id={"kv": jnp.int32(j)},
            device_id_type=MESH,
        )

    def attend(r):
        shards = LAST[r] + 1
        span = shards * ROWS
        length = len_of[r]
        head = jnp.int32(0)
        for h in range(n_head):
            head = head + (me == PLACE[r][h]).astype(jnp.int32) * h

        pw_keys = jnp.concatenate([pw_ref[0].T] * (ROWS // L_CMP), axis=1)
        pw_vals = jnp.concatenate([pw_ref[1].T] * (ROWS // L_CMP), axis=1)
        weight[...] = jnp.concatenate([pw_keys, pw_vals], axis=0)
        lane_blk = iota((ROWS, ROWS), 0) // L_CMP
        lane_col = iota((ROWS, ROWS), 1)

        def prepare(j):
            @pl.when(me != j)
            def _():
                arrival(r, j).wait_recv()

            cols = slice(j * ROWS, (j + 1) * ROWS)
            q_ext[0:HD, cols] = recv[r, j, QUER:EXTRA, :]
            k_ext[0:HD, cols] = recv[r, j, KEYS:VALS, :]
            v_all[0:HD, cols] = recv[r, j, VALS:QUER, :]
            picks = recv[r, j, EXTRA:MSG, :].astype(F32)
            blocks = iota((32, ROWS), 0).astype(F32)
            hit = blocks == picks[8:9]
            for t in range(1, 8):
                hit = hit | (blocks == picks[8 + t : 9 + t])
            q_ext[HD : HD + 32, cols] = jnp.where(hit, 0.0, NEG).astype(BF)
            one_row = (iota((32, ROWS), 0) == 0).astype(F32)
            q_ext[HD + 32 :, cols] = one_row.astype(BF)
            key = j * ROWS + iota((32, ROWS), 1)
            k_ext[HD : HD + 32, cols] = (iota((32, ROWS), 0) == key // QB).astype(F32).astype(BF)
            k_ext[HD + 32 :, cols] = jnp.where(key >= length, one_row * NEG, 0.0).astype(BF)
            v_all[HD:, cols] = (iota((HD, ROWS), 0) == 0).astype(F32).astype(BF)
            prod = recv[r, j, KEYS:QUER, :].astype(F32) * weight[...]
            hi = prod.astype(BF)
            lo = (prod - hi.astype(F32)).astype(BF)
            group = jnp.where(lane_col == j * (ROWS // L_CMP) + lane_blk, 1.0, 0.0).astype(BF)
            return [hi, lo], [group, group]

        pool_sum[...] = jnp.zeros((2 * HD, ROWS), F32)
        for t in range(span // TILE):
            lo, hi = t * TILE, (t + 1) * TILE
            lefts, rights = [], []
            for i in range(TILE // ROWS):
                left_i, right_i = prepare(t * (TILE // ROWS) + i)
                lefts, rights = lefts + left_i, rights + right_i
            fresh = nn(jnp.concatenate(lefts, axis=1), jnp.concatenate(rights, axis=0))
            known = lane_col < t * (TILE // L_CMP)
            pool_sum[...] = jnp.where(known, pool_sum[...], fresh)
            pooled = pool_sum[...].astype(BF)
            key_pooled = jnp.concatenate([pooled[:HD], jnp.zeros((HD, ROWS), BF)], axis=0)
            val_pooled = pooled[HD:]
            q = q_ext[:, lo:hi].T
            scores = nn(q, k_ext[:, :hi])
            edge = jnp.where(
                iota((TILE, TILE), 1) <= iota((TILE, TILE), 0), scores[:, lo:hi], NEG
            )
            scores = edge if t == 0 else jnp.concatenate([scores[:, :lo], edge], axis=1)
            top = jnp.max(scores, axis=1, keepdims=True)
            e = jnp.exp(scores - top)
            summed = nt(e.astype(BF), v_all[:, :hi])
            picked_out = summed[:, :HD] / summed[:, HD : HD + 1]

            scores = nn(q, key_pooled)
            pos = lo + iota((TILE, ROWS), 0)
            end = iota((TILE, ROWS), 1) * L_CMP + (L_CMP - 1)
            usable = (end <= pos) & (end < length)
            top = jnp.max(jnp.where(usable, scores, NEG), axis=1, keepdims=True)
            e = jnp.where(usable, jnp.exp(jnp.where(usable, scores, NEG) - top), 0.0)
            tot = jnp.sum(e, axis=1, keepdims=True)
            pooled_out = nt(e.astype(BF), val_pooled) / jnp.where(tot > 0, tot, 1.0)

            both = jnp.concatenate([pooled_out, picked_out], axis=1).T
            for i in range(TILE // ROWS):
                j = t * (TILE // ROWS) + i
                g = recv[r, j, EXTRA:MSG, :].astype(F32)
                part = both[:, i * ROWS : (i + 1) * ROWS]
                mix = (g[0:1] + g[2:3]) * part[:HD] + (g[1:2] + g[3:4]) * part[HD:]
                alive = j * ROWS + iota((HD, ROWS), 1) < length
                o_stage[r, j] = jnp.where(alive, mix, 0.0).astype(BF)

                if j not in PAIRED:
                    before = RANK_ORDER[: RANK_ORDER.index(r)]
                    new = [
                        p
                        for p in PLACE[r]
                        if p < j and not any(p in PLACE[q] and j <= LAST[q] for q in before)
                    ]

                    @pl.when(any_of(me, new))
                    def _():
                        pl.semaphore_wait(ready_kv.at[j], 1)

                @pl.when(me != j)
                def _():
                    returned(r, head, j).start()

                @pl.when(me == j)
                def _():
                    a_buf[r, head] = o_stage[r, j]

    for r in RANK_ORDER:

        @pl.when(any_of(me, PLACE[r]))
        def _():
            attend(r)

    half = ROWS // 2
    lower, upper = pl.ds(0, half), pl.ds(half, half)

    def hop(r, block, rows, to, n):
        ref = x_buf.at[r, block] if rows is None else x_buf.at[r, block, rows]
        return pltpu.make_async_remote_copy(
            src_ref=ref,
            dst_ref=ref,
            send_sem=g_send.at[r],
            recv_sem=g_recv.at[r, RELAY_SEM[n]],
            device_id={"tp": to},
            device_id_type=MESH,
        )

    def sent(r, n):
        return hop(r, *(
            (tp, lower, right, 0),
            (tp, upper, right, 1),
            (tp, upper, left, 2),
            (tp, lower, left, 3),
            (left, lower, right, 4),
            (right, upper, left, 5),
            (tp, None, partner, 6),
            (left, None, partner, 7),
            (right, None, partner, 8),
            (far, None, partner, 9),
        )[n])

    def other(t):
        return t + 1 - 2 * lax.rem(t, 2)

    def received(r, n):
        return hop(r, *(
            (left, lower, left, 0),
            (left, upper, left, 1),
            (right, upper, right, 2),
            (right, lower, right, 3),
            (far, lower, left, 4),
            (far, upper, right, 5),
            (other(tp), None, partner, 6),
            (other(left), None, partner, 7),
            (other(right), None, partner, 8),
            (other(far), None, partner, 9),
        )[n])

    rows_each = ROWS // n_tp
    width = wo.shape[1]

    def column_copy(r, to):
        return pltpu.make_async_remote_copy(
            src_ref=y_buf.at[r, pl.ds(pl.multiple_of(to * rows_each, rows_each), rows_each)],
            dst_ref=o_buf.at[r, :, pl.ds(pl.multiple_of(tp * width, width), width)],
            send_sem=y_send.at[r],
            recv_sem=y_recv.at[r],
            device_id={"tp": to},
            device_id_type=MESH,
        )

    def columns_all(r):
        rest = pl.ds(0, (n_tp - 1) * rows_each)
        return pltpu.make_async_remote_copy(
            src_ref=y_buf.at[r, rest],
            dst_ref=y_buf.at[r, rest],
            send_sem=y_send.at[r],
            recv_sem=y_recv.at[r],
            device_id={"tp": partner},
            device_id_type=MESH,
        )

    loads[8].wait()
    for t in range(n_tp):

        @pl.when(tp > t)
        def _():
            pl.semaphore_wait(ready_tp.at[t], 1)


    def handed_back(r, count):
        return pltpu.make_async_remote_copy(
            src_ref=o_stage.at[r, pl.ds(0, count)],
            dst_ref=a_buf.at[r, pl.ds(0, count)],
            send_sem=o_send.at[r],
            recv_sem=o_recv.at[r],
            device_id={"kv": jnp.int32(0)},
            device_id_type=MESH,
        )

    def own(r):
        inside = any_of(me, PLACE[r])

        @pl.when(inside)
        def _():
            handed_back(r, n_head - 1).wait_recv()

        @pl.when(jnp.logical_not(inside))
        def _():
            handed_back(r, n_head).wait_recv()

        x_buf[r, tp] = a_buf[r].reshape(n_head * HD, ROWS).T
        for n in (0, 2, 1, 3, 6):
            sent(r, n).start()

    def relay(r):
        received(r, 0).wait_recv()
        sent(r, 4).start()
        received(r, 2).wait_recv()
        sent(r, 5).start()
        received(r, 1).wait_recv()
        sent(r, 7).start()
        received(r, 3).wait_recv()
        sent(r, 8).start()

    def across(r):
        hop(r, far, None, left, 4).wait_recv()
        sent(r, 9).start()

    def mix(r):
        blocks = x_buf.at[r, pl.ds(0, n_tp // 2)]
        pltpu.make_async_remote_copy(
            src_ref=blocks,
            dst_ref=blocks,
            send_sem=g_send.at[r],
            recv_sem=g_recv.at[r, RELAY_SEM[6]],
            device_id={"tp": partner},
            device_id_type=MESH,
        ).wait_recv()
        rows = jnp.concatenate([x_buf[r, g] for g in range(n_tp)], axis=1)
        y_buf[r] = nn(rows, wo[...]).astype(BF)
        for step in range(1, n_tp):
            column_copy(r, lax.rem(tp + step, n_tp)).start()
        mine = pl.ds(pl.multiple_of(tp * rows_each, rows_each), rows_each)
        o_buf[r, :, pl.ds(pl.multiple_of(tp * width, width), width)] = y_buf[r, mine]

    def stage(step, r):
        @pl.when(me <= LAST[r])
        def _():
            step(r)

    first, second, third, last = RANK_ORDER
    for step, r in (
        (own, first), (own, second), (relay, first), (own, third), (relay, second), (own, last),
        (across, first), (relay, third), (across, second), (mix, first), (relay, last),
        (across, third), (mix, second), (across, last), (mix, third), (mix, last),
    ):
        stage(step, r)

    for r in range(n_seq):

        @pl.when(me > LAST[r])
        def _():
            o_buf[r] = jnp.zeros(o_buf.shape[1:], BF)

    for r in range(n_seq):

        @pl.when(me <= LAST[r])
        def _():
            columns_all(r).wait_recv()

    many = rows_each * n_seq
    want = iota((many, many), 0)
    have = iota((many, many), 1)
    pick = jnp.zeros((many, many), F32)
    for r in range(n_seq):
        hit = (have == r * rows_each + want // n_seq) & (lax.rem(want, n_seq) == seq_of[r])
        pick = jnp.where(hit, 1.0, pick)
    pick = pick.astype(BF)
    for c in range(n_tp):
        cols = slice(c * width, (c + 1) * width)
        rows = o_buf[:, :, cols].reshape(many, width)
        out_ref[:, :, cols] = nn(pick, rows).astype(BF).reshape(rows_each, n_seq, width)

    for r in range(n_seq):
        inside = any_of(me, PLACE[r])

        @pl.when((me <= LAST[r]) & inside)
        def _():
            departures(r, n_head - 1).wait_send()

        @pl.when((me <= LAST[r]) & jnp.logical_not(inside))
        def _():
            departures(r, n_head).wait_send()

        def returned_all(count):
            return pltpu.make_async_remote_copy(
                src_ref=o_stage.at[r, pl.ds(0, count)],
                dst_ref=o_stage.at[r, pl.ds(0, count)],
                send_sem=o_send.at[r],
                recv_sem=o_recv.at[r],
                device_id={"kv": jnp.int32(0)},
                device_id_type=MESH,
            )

        @pl.when(inside & (me <= LAST[r]))
        def _():
            returned_all(LAST[r]).wait_send()

        if any(p > LAST[r] for p in PLACE[r]):

            @pl.when(inside & (me > LAST[r]))
            def _():
                returned_all(LAST[r] + 1).wait_send()

        @pl.when(me <= LAST[r])
        def _():
            blocks = x_buf.at[r, pl.ds(0, 2 + 1 + n_tp // 2)]
            pltpu.make_async_remote_copy(
                src_ref=blocks,
                dst_ref=blocks,
                send_sem=g_send.at[r],
                recv_sem=g_recv.at[r, 0],
                device_id={"tp": partner},
                device_id_type=MESH,
            ).wait_send()
            columns_all(r).wait_send()


def body(tokens, lengths, chosen, w_query, w_key, w_value, w_gate, pool_weights, w_out):
    rows, n_seq, depth = tokens.shape
    n_head = w_query.shape[1] // HD
    n_kv, n_tp = lax.axis_size("kv"), lax.axis_size("tp")
    gate_rows = jnp.transpose(w_gate, (1, 2, 0))
    width = w_out.shape[1]
    total = rows * n_seq
    vmem = pl.BlockSpec(memory_space=pltpu.VMEM)
    hbm = pl.BlockSpec(memory_space=pl.ANY)
    dma = pltpu.SemaphoreType.DMA
    full = n_kv * rows

    def whole(*refs):
        kernel(n_kv, n_tp, n_seq, n_head, *refs)

    return pl.pallas_call(
        whole,
        out_shape=jax.ShapeDtypeStruct((rows // n_tp, n_seq, n_tp * width), BF),
        in_specs=[hbm] * 9,
        out_specs=vmem,
        scratch_shapes=[
            pltpu.VMEM((rows, n_seq, depth), BF),
            pltpu.VMEM((total, depth), BF),
            pltpu.VMEM((3, depth, n_head * HD), BF),
            pltpu.VMEM(gate_rows.shape, BF),
            pltpu.VMEM(pool_weights.shape, F32),
            pltpu.VMEM(w_out.shape, BF),
            pltpu.SMEM(lengths.shape, jnp.int32),
            pltpu.SMEM(chosen.shape, jnp.int32),
            pltpu.VMEM((total, total), BF),
            pltpu.VMEM((n_seq * n_head, MSG, rows), BF),
            pltpu.VMEM((n_seq, n_kv, MSG, rows), BF),
            pltpu.VMEM((128, full), BF),
            pltpu.VMEM((128, full), BF),
            pltpu.VMEM((128, full), BF),
            pltpu.VMEM((2 * HD, rows), F32),
            pltpu.VMEM((2 * HD, rows), F32),
            pltpu.VMEM((n_seq, n_kv, HD, rows), BF),
            pltpu.VMEM((n_seq, n_head, HD, rows), BF),
            pltpu.VMEM((n_seq, n_tp, rows, n_head * HD), BF),
            pltpu.VMEM((n_seq, rows, width), BF),
            pltpu.VMEM((n_seq, rows // n_tp, n_tp * width), BF),
            dma((9,)),
            dma((n_seq,)),
            dma((FIRST[-1] + LAST[-1] + 1,)),
            dma((n_seq,)),
            dma((n_seq,)),
            dma((n_seq,)),
            dma((n_seq, 6)),
            dma((n_seq,)),
            dma((n_seq,)),
            pltpu.SemaphoreType.REGULAR((n_kv,)),
            pltpu.SemaphoreType.REGULAR((n_tp,)),
        ],
        compiler_params=pltpu.CompilerParams(
            collective_id=0, has_side_effects=True, vmem_limit_bytes=60 * 2**20
        ),
    )(tokens, lengths, chosen, w_query, w_key, w_value, gate_rows, pool_weights, w_out)


def solution(mesh):
    placed = (
        P("kv", "grp", None),
        P("grp"),
        P("grp", "tp", "kv", None),
        P(None, "tp"),
        P(None, "tp"),
        P(None, "tp"),
        P(None, None, "tp"),
        P(),
        P(None, "tp"),
    )
    return jax.shard_map(
        body, mesh=mesh, in_specs=placed, out_specs=P(("kv", "tp"), "grp", None), check_vma=False
    )
```

```python
import jax
import jax.numpy as jnp
from jax import lax
from jax.experimental import pallas as pl
from jax.experimental.pallas import tpu as pltpu
from jax.sharding import PartitionSpec as P

HD = 64
QB = 64
L_CMP = 32
NEG = -1e30
BF = jnp.bfloat16
F32 = jnp.float32
MESH = pl.DeviceIdType.MESH

ROWS = 128
AUX = 16
MSG = 3 * HD + AUX
KEYS, VALS, QUER, EXTRA = 0, HD, 2 * HD, 3 * HD
LAST = (15, 11, 7, 5)
PLACE = (
    (9, 11, 12, 13),
    (4, 5, 6, 7),
    (3, 4, 1, 2),
    (2, 3, 1, 5),
)
RANK_ORDER = (3, 2, 1, 0)
TILE = 256
AHEAD = 2
NEAR = 4
RELAY_SEM = (0, 1, 2, 3, 4, 4, 5, 5, 5, 5)
SHARDS = LAST[0] + 1
PAIRED = sorted({p for places in PLACE for p in places})


def returns_to(i, j):
    return any(i in PLACE[r] and j <= LAST[r] for r in range(len(PLACE)))


def sends_to(i, j):
    asked = any(j in PLACE[r] and i <= LAST[r] for r in range(len(PLACE)))
    return asked or returns_to(i, j)


FIRST = [sum(LAST[:r]) + r for r in range(len(LAST))]


def any_of(me, places):
    here = me < 0
    for p in places:
        here = here | (me == p)
    return here


def iota(shape, dim):
    return lax.broadcasted_iota(jnp.int32, shape, dim)


def nt(a, b):
    return lax.dot_general(a, b, (((1,), (1,)), ((), ())), preferred_element_type=F32)


def nn(a, b):
    return jnp.dot(a, b, preferred_element_type=F32)


def kernel(
    n_kv, n_tp, n_seq, n_head,
    tok_hbm, len_hbm, chosen_hbm, wq_hbm, wk_hbm, wv_hbm, wg_hbm, pw_hbm, wo_hbm,
    out_ref,
    tok, flat, w_buf, wg, pw_ref, wo, len_ref, chosen_ref,
    sel_t, send, recv, k_ext, q_ext, v_all, weight, pool_sum, o_stage, a_buf, x_buf, y_buf, o_buf,
    load_sem, q_send, q_recv, o_send, o_recv, g_send, g_recv, y_send, y_recv,
    ready_kv, ready_tp,
):
    me = lax.axis_index("kv")
    tp = lax.axis_index("tp")
    chips = n_tp // 2
    core = lax.rem(tp, 2)
    chip = tp // 2
    right = lax.rem(chip + 1, chips) * 2 + core
    left = lax.rem(chip + chips - 1, chips) * 2 + core
    far = lax.rem(chip + 2, chips) * 2 + core
    partner = chip * 2 + 1 - core

    barrier = pltpu.get_barrier_semaphore()
    for j in range(n_kv):

        if j == 0:
            tells = (me > 0) & (me < NEAR)
        elif j < NEAR:
            tells = (me > 0) & (me < j)
        else:
            tells = me < j

        @pl.when(tells)
        def _():
            pl.semaphore_signal(
                barrier, inc=1, device_id={"kv": jnp.int32(j)}, device_id_type=MESH
            )

    for t in range(n_tp):

        @pl.when(tp > t)
        def _():
            pl.semaphore_signal(
                barrier, inc=1, device_id={"tp": jnp.int32(t)}, device_id_type=MESH
            )

    loads = [
        pltpu.make_async_copy(len_hbm, len_ref, load_sem.at[0]),
        pltpu.make_async_copy(tok_hbm, tok, load_sem.at[1]),
        pltpu.make_async_copy(wk_hbm, w_buf.at[0], load_sem.at[2]),
        pltpu.make_async_copy(wv_hbm, w_buf.at[1], load_sem.at[3]),
        pltpu.make_async_copy(wq_hbm, w_buf.at[2], load_sem.at[4]),
        pltpu.make_async_copy(wg_hbm, wg, load_sem.at[5]),
        pltpu.make_async_copy(chosen_hbm, chosen_ref, load_sem.at[6]),
        pltpu.make_async_copy(pw_hbm, pw_ref, load_sem.at[7]),
        pltpu.make_async_copy(wo_hbm, wo, load_sem.at[8]),
    ]
    for copy in loads:
        copy.start()
    near = (me > 0) & (me < NEAR)
    told = me + n_tp - 1 - tp - near.astype(jnp.int32) + (me == 0).astype(jnp.int32) * (NEAR - 1)

    def enter():
        @pl.when(told > 0)
        def _():
            pl.semaphore_wait(barrier, told)

        for i in range(n_kv):
            first = NEAR if i == 0 else i + 1
            later = [j for j in range(first, n_kv) if sends_to(i, j)]

            @pl.when(any_of(me, later))
            def _():
                pl.semaphore_signal(
                    ready_kv.at[me], inc=1, device_id={"kv": jnp.int32(i)}, device_id_type=MESH
                )

        for t in range(n_tp):

            @pl.when(tp < t)
            def _():
                pl.semaphore_signal(
                    ready_tp.at[tp], inc=1, device_id={"tp": jnp.int32(t)}, device_id_type=MESH
                )

    pl.when(near)(enter)
    loads[0].wait()

    lens = [len_ref[s] for s in range(n_seq)]
    ranks = []
    for s in range(n_seq):
        rank = jnp.int32(0)
        for o in range(n_seq):
            if o != s:
                ahead = (lens[o] >= lens[s]) if o < s else (lens[o] > lens[s])
                rank = rank + ahead.astype(jnp.int32)
        ranks.append(rank)
    seq_of, len_of = [], []
    for r in range(n_seq):
        seq, length = jnp.int32(0), jnp.int32(0)
        for s in range(n_seq):
            hit = (ranks[s] == r).astype(jnp.int32)
            seq = seq + hit * s
            length = length + hit * lens[s]
        seq_of.append(seq)
        len_of.append(length)

    total = ROWS * n_seq
    row = iota((total, ROWS), 0)
    col = iota((total, ROWS), 1)
    for r in range(n_seq):
        hit = row == col * n_seq + seq_of[r]
        sel_t[:, r * ROWS : (r + 1) * ROWS] = jnp.where(hit, 1.0, 0.0).astype(BF)

    loads[1].wait()
    flat[...] = tok[...].reshape(flat.shape)

    def project(slot, base):
        loads[2 + slot].wait()
        made = nn(flat[...], w_buf[slot]).astype(BF).T
        placed = nn(made, sel_t[...])
        if base == QUER:
            placed = placed * HD**-0.5
        placed = placed.astype(BF)
        for r in range(n_seq):
            for h in range(n_head):
                send[r * n_head + h, base : base + HD, :] = placed[
                    h * HD : (h + 1) * HD, r * ROWS : (r + 1) * ROWS
                ]

    def extras():
        loads[5].wait()
        loads[6].wait()
        gates = jax.nn.sigmoid(nt(wg[...].reshape(2 * n_head, wg.shape[2]), flat[...]))
        gate_hi = gates.astype(BF)
        gate_lo = (gates - gate_hi.astype(F32)).astype(BF)
        gate_rows = nn(jnp.concatenate([gate_hi, gate_lo], axis=0), sel_t[...])
        n_blk, top = chosen_ref.shape[2:]
        slot = iota((top, ROWS), 0)
        blk = iota((top, ROWS), 1) // (ROWS // n_blk)
        for r in range(n_seq):
            cols = slice(r * ROWS, (r + 1) * ROWS)
            for h in range(n_head):
                picked = jnp.zeros((top, ROWS), jnp.int32)
                for b in range(n_blk):
                    for t in range(top):
                        at = (slot == t) & (blk == b)
                        picked = jnp.where(at, chosen_ref[seq_of[r], h, b, t], picked)
                kinds = [
                    gate_rows[g * n_head + h : g * n_head + h + 1, cols] for g in range(4)
                ]
                rest = jnp.zeros((AUX - top - 4, ROWS), F32)
                aux = jnp.concatenate([*kinds, rest, picked.astype(F32)], axis=0)
                send[r * n_head + h, EXTRA:, :] = aux.astype(BF)

    wholes = ((0, MSG),)
    halves = ((0, QUER), (QUER, MSG - QUER))
    thirds = ((KEYS, HD), (VALS, HD), (QUER, MSG - QUER))
    parts_of = {3: thirds, 2: thirds, 1: halves, 0: wholes}

    def message(r, h, part):
        rows = pl.ds(*parts_of[r][part])
        return pltpu.make_async_remote_copy(
            src_ref=send.at[r * n_head + h, rows],
            dst_ref=recv.at[r, me, rows],
            send_sem=q_send.at[r],
            recv_sem=q_recv.at[FIRST[r] + me],
            device_id={"kv": jnp.int32(PLACE[r][h])},
            device_id_type=MESH,
        )

    def arrival(r, j):
        return pltpu.make_async_remote_copy(
            src_ref=send.at[0],
            dst_ref=recv.at[r, j],
            send_sem=q_send.at[r],
            recv_sem=q_recv.at[FIRST[r] + j],
            device_id={"kv": jnp.int32(0)},
            device_id_type=MESH,
        )

    def departures(r, count):
        return pltpu.make_async_remote_copy(
            src_ref=send.at[pl.ds(0, count)],
            dst_ref=send.at[pl.ds(0, count)],
            send_sem=q_send.at[r],
            recv_sem=q_recv.at[0],
            device_id={"kv": jnp.int32(0)},
            device_id_type=MESH,
        )

    def await_ready(there):
        first = 1 if there < NEAR else 0

        @pl.when(any_of(me, [i for i in range(first, there) if sends_to(i, there)]))
        def _():
            pl.semaphore_wait(ready_kv.at[there], 1)

    asked = set()

    def send_rank(r, part):
        for h in sorted(range(n_head), key=lambda h: PLACE[r][h]):
            there = PLACE[r][h]
            if there not in asked:
                asked.add(there)
                await_ready(there)

            @pl.when((me <= LAST[r]) & (me != there))
            def _():
                message(r, h, part).start()

    ahead = me < AHEAD
    project(0, KEYS)
    pl.when(me >= NEAR)(enter)

    @pl.when(jnp.logical_not(ahead))
    def _():
        send_rank(3, 0)
        send_rank(2, 0)

    project(1, VALS)
    pl.when(me == 0)(enter)

    def send_to(there, wanted):
        for r in (3, 2, 1, 0):
            for h in range(n_head):
                if PLACE[r][h] == there:
                    for part in wanted(r):

                        @pl.when(me != there)
                        def _():
                            message(r, h, part).start()

    @pl.when(jnp.logical_not(ahead))
    def _():
        send_rank(3, 1)
        send_rank(2, 1)

    @pl.when(ahead)
    def _():
        for there in PAIRED:
            if there < NEAR:
                await_ready(there)
                send_to(there, lambda r: range(len(parts_of[r]) - 1))

    project(2, QUER)

    @pl.when(jnp.logical_not(ahead))
    def _():
        send_rank(1, 0)

    extras()
    for r in range(n_seq):
        for h in range(n_head):
            there = PLACE[r][h]
            if there <= LAST[r]:

                @pl.when(me == there)
                def _():
                    recv[r, there] = send[r * n_head + h]

    @pl.when(ahead)
    def _():
        for there in PAIRED:
            if there < NEAR:
                send_to(there, lambda r: [len(parts_of[r]) - 1])
        for there in PAIRED:
            if there >= NEAR:
                await_ready(there)
                send_to(there, lambda r: range(len(parts_of[r])))

    @pl.when(jnp.logical_not(ahead))
    def _():
        send_rank(3, 2)
        send_rank(2, 2)
        send_rank(1, 1)
        send_rank(0, 0)

    loads[7].wait()

    def returned(r, h_here, j):
        return pltpu.make_async_remote_copy(
            src_ref=o_stage.at[r, j],
            dst_ref=a_buf.at[r, h_here],
            send_sem=o_send.at[r],
            recv_sem=o_recv.at[r],
            device_id={"kv": jnp.int32(j)},
            device_id_type=MESH,
        )

    def attend(r):
        shards = LAST[r] + 1
        span = shards * ROWS
        length = len_of[r]
        head = jnp.int32(0)
        for h in range(n_head):
            head = head + (me == PLACE[r][h]).astype(jnp.int32) * h

        pw_keys = jnp.concatenate([pw_ref[0].T] * (ROWS // L_CMP), axis=1)
        pw_vals = jnp.concatenate([pw_ref[1].T] * (ROWS // L_CMP), axis=1)
        weight[...] = jnp.concatenate([pw_keys, pw_vals], axis=0)
        lane_blk = iota((ROWS, ROWS), 0) // L_CMP
        lane_col = iota((ROWS, ROWS), 1)

        def prepare(j):
            @pl.when(me != j)
            def _():
                arrival(r, j).wait_recv()

            cols = slice(j * ROWS, (j + 1) * ROWS)
            q_ext[0:HD, cols] = recv[r, j, QUER:EXTRA, :]
            k_ext[0:HD, cols] = recv[r, j, KEYS:VALS, :]
            v_all[0:HD, cols] = recv[r, j, VALS:QUER, :]
            picks = recv[r, j, EXTRA:MSG, :].astype(F32)
            blocks = iota((32, ROWS), 0).astype(F32)
            hit = blocks == picks[8:9]
            for t in range(1, 8):
                hit = hit | (blocks == picks[8 + t : 9 + t])
            q_ext[HD : HD + 32, cols] = jnp.where(hit, 0.0, NEG).astype(BF)
            one_row = (iota((32, ROWS), 0) == 0).astype(F32)
            q_ext[HD + 32 :, cols] = one_row.astype(BF)
            key = j * ROWS + iota((32, ROWS), 1)
            k_ext[HD : HD + 32, cols] = (iota((32, ROWS), 0) == key // QB).astype(F32).astype(BF)
            k_ext[HD + 32 :, cols] = jnp.where(key >= length, one_row * NEG, 0.0).astype(BF)
            v_all[HD:, cols] = (iota((HD, ROWS), 0) == 0).astype(F32).astype(BF)
            prod = recv[r, j, KEYS:QUER, :].astype(F32) * weight[...]
            hi = prod.astype(BF)
            lo = (prod - hi.astype(F32)).astype(BF)
            group = jnp.where(lane_col == j * (ROWS // L_CMP) + lane_blk, 1.0, 0.0).astype(BF)
            return [hi, lo], [group, group]

        pool_sum[...] = jnp.zeros((2 * HD, ROWS), F32)
        for t in range(span // TILE):
            lo, hi = t * TILE, (t + 1) * TILE
            lefts, rights = [], []
            for i in range(TILE // ROWS):
                left_i, right_i = prepare(t * (TILE // ROWS) + i)
                lefts, rights = lefts + left_i, rights + right_i
            fresh = nn(jnp.concatenate(lefts, axis=1), jnp.concatenate(rights, axis=0))
            known = lane_col < t * (TILE // L_CMP)
            pool_sum[...] = jnp.where(known, pool_sum[...], fresh)
            pooled = pool_sum[...].astype(BF)
            key_pooled = jnp.concatenate([pooled[:HD], jnp.zeros((HD, ROWS), BF)], axis=0)
            val_pooled = pooled[HD:]
            q = q_ext[:, lo:hi].T
            scores = nn(q, k_ext[:, :hi])
            edge = jnp.where(
                iota((TILE, TILE), 1) <= iota((TILE, TILE), 0), scores[:, lo:hi], NEG
            )
            scores = edge if t == 0 else jnp.concatenate([scores[:, :lo], edge], axis=1)
            top = jnp.max(scores, axis=1, keepdims=True)
            e = jnp.exp(scores - top)
            summed = nt(e.astype(BF), v_all[:, :hi])
            picked_out = summed[:, :HD] / summed[:, HD : HD + 1]

            scores = nn(q, key_pooled)
            pos = lo + iota((TILE, ROWS), 0)
            end = iota((TILE, ROWS), 1) * L_CMP + (L_CMP - 1)
            usable = (end <= pos) & (end < length)
            top = jnp.max(jnp.where(usable, scores, NEG), axis=1, keepdims=True)
            e = jnp.where(usable, jnp.exp(jnp.where(usable, scores, NEG) - top), 0.0)
            tot = jnp.sum(e, axis=1, keepdims=True)
            pooled_out = nt(e.astype(BF), val_pooled) / jnp.where(tot > 0, tot, 1.0)

            both = jnp.concatenate([pooled_out, picked_out], axis=1).T
            for i in range(TILE // ROWS):
                j = t * (TILE // ROWS) + i
                g = recv[r, j, EXTRA:MSG, :].astype(F32)
                part = both[:, i * ROWS : (i + 1) * ROWS]
                mix = (g[0:1] + g[2:3]) * part[:HD] + (g[1:2] + g[3:4]) * part[HD:]
                alive = j * ROWS + iota((HD, ROWS), 1) < length
                o_stage[r, j] = jnp.where(alive, mix, 0.0).astype(BF)

                if j not in PAIRED:
                    before = RANK_ORDER[: RANK_ORDER.index(r)]
                    new = [
                        p
                        for p in PLACE[r]
                        if p < j and not any(p in PLACE[q] and j <= LAST[q] for q in before)
                    ]

                    @pl.when(any_of(me, new))
                    def _():
                        pl.semaphore_wait(ready_kv.at[j], 1)

                @pl.when(me != j)
                def _():
                    returned(r, head, j).start()

                @pl.when(me == j)
                def _():
                    a_buf[r, head] = o_stage[r, j]

    for r in RANK_ORDER:

        @pl.when(any_of(me, PLACE[r]))
        def _():
            attend(r)

    half = ROWS // 2
    lower, upper = pl.ds(0, half), pl.ds(half, half)

    def hop(r, block, rows, to, n):
        ref = x_buf.at[r, block] if rows is None else x_buf.at[r, block, rows]
        return pltpu.make_async_remote_copy(
            src_ref=ref,
            dst_ref=ref,
            send_sem=g_send.at[r],
            recv_sem=g_recv.at[r, RELAY_SEM[n]],
            device_id={"tp": to},
            device_id_type=MESH,
        )

    def sent(r, n):
        return hop(r, *(
            (tp, lower, right, 0),
            (tp, upper, right, 1),
            (tp, upper, left, 2),
            (tp, lower, left, 3),
            (left, lower, right, 4),
            (right, upper, left, 5),
            (tp, None, partner, 6),
            (left, None, partner, 7),
            (right, None, partner, 8),
            (far, None, partner, 9),
        )[n])

    def other(t):
        return t + 1 - 2 * lax.rem(t, 2)

    def received(r, n):
        return hop(r, *(
            (left, lower, left, 0),
            (left, upper, left, 1),
            (right, upper, right, 2),
            (right, lower, right, 3),
            (far, lower, left, 4),
            (far, upper, right, 5),
            (other(tp), None, partner, 6),
            (other(left), None, partner, 7),
            (other(right), None, partner, 8),
            (other(far), None, partner, 9),
        )[n])

    rows_each = ROWS // n_tp
    width = wo.shape[1]

    def column_copy(r, to):
        return pltpu.make_async_remote_copy(
            src_ref=y_buf.at[r, pl.ds(pl.multiple_of(to * rows_each, rows_each), rows_each)],
            dst_ref=o_buf.at[r, :, pl.ds(pl.multiple_of(tp * width, width), width)],
            send_sem=y_send.at[r],
            recv_sem=y_recv.at[r],
            device_id={"tp": to},
            device_id_type=MESH,
        )

    def columns_all(r):
        rest = pl.ds(0, (n_tp - 1) * rows_each)
        return pltpu.make_async_remote_copy(
            src_ref=y_buf.at[r, rest],
            dst_ref=y_buf.at[r, rest],
            send_sem=y_send.at[r],
            recv_sem=y_recv.at[r],
            device_id={"tp": partner},
            device_id_type=MESH,
        )

    loads[8].wait()
    for t in range(n_tp):

        @pl.when(tp > t)
        def _():
            pl.semaphore_wait(ready_tp.at[t], 1)


    def handed_back(r, count):
        return pltpu.make_async_remote_copy(
            src_ref=o_stage.at[r, pl.ds(0, count)],
            dst_ref=a_buf.at[r, pl.ds(0, count)],
            send_sem=o_send.at[r],
            recv_sem=o_recv.at[r],
            device_id={"kv": jnp.int32(0)},
            device_id_type=MESH,
        )

    def own(r):
        inside = any_of(me, PLACE[r])

        @pl.when(inside)
        def _():
            handed_back(r, n_head - 1).wait_recv()

        @pl.when(jnp.logical_not(inside))
        def _():
            handed_back(r, n_head).wait_recv()

        x_buf[r, tp] = a_buf[r].reshape(n_head * HD, ROWS).T
        for n in (0, 2, 1, 3, 6):
            sent(r, n).start()

    def relay(r):
        received(r, 0).wait_recv()
        sent(r, 4).start()
        received(r, 2).wait_recv()
        sent(r, 5).start()
        received(r, 1).wait_recv()
        sent(r, 7).start()
        received(r, 3).wait_recv()
        sent(r, 8).start()

    def across(r):
        hop(r, far, None, left, 4).wait_recv()
        sent(r, 9).start()

    def mix(r):
        blocks = x_buf.at[r, pl.ds(0, n_tp // 2)]
        pltpu.make_async_remote_copy(
            src_ref=blocks,
            dst_ref=blocks,
            send_sem=g_send.at[r],
            recv_sem=g_recv.at[r, RELAY_SEM[6]],
            device_id={"tp": partner},
            device_id_type=MESH,
        ).wait_recv()
        rows = jnp.concatenate([x_buf[r, g] for g in range(n_tp)], axis=1)
        y_buf[r] = nn(rows, wo[...]).astype(BF)
        for step in range(1, n_tp):
            column_copy(r, lax.rem(tp + step, n_tp)).start()
        mine = pl.ds(pl.multiple_of(tp * rows_each, rows_each), rows_each)
        o_buf[r, :, pl.ds(pl.multiple_of(tp * width, width), width)] = y_buf[r, mine]

    def stage(step, r):
        @pl.when(me <= LAST[r])
        def _():
            step(r)

    first, second, third, last = RANK_ORDER
    for step, r in (
        (own, first), (own, second), (relay, first), (own, third), (relay, second), (own, last),
        (across, first), (relay, third), (across, second), (mix, first), (relay, last),
        (across, third), (mix, second), (across, last), (mix, third), (mix, last),
    ):
        stage(step, r)

    for r in range(n_seq):

        @pl.when(me > LAST[r])
        def _():
            o_buf[r] = jnp.zeros(o_buf.shape[1:], BF)

    for r in range(n_seq):

        @pl.when(me <= LAST[r])
        def _():
            columns_all(r).wait_recv()

    many = rows_each * n_seq
    want = iota((many, many), 0)
    have = iota((many, many), 1)
    pick = jnp.zeros((many, many), F32)
    for r in range(n_seq):
        hit = (have == r * rows_each + want // n_seq) & (lax.rem(want, n_seq) == seq_of[r])
        pick = jnp.where(hit, 1.0, pick)
    pick = pick.astype(BF)
    for c in range(n_tp):
        cols = slice(c * width, (c + 1) * width)
        rows = o_buf[:, :, cols].reshape(many, width)
        out_ref[:, :, cols] = nn(pick, rows).astype(BF).reshape(rows_each, n_seq, width)

    for r in range(n_seq):
        inside = any_of(me, PLACE[r])

        @pl.when((me <= LAST[r]) & inside)
        def _():
            departures(r, n_head - 1).wait_send()

        @pl.when((me <= LAST[r]) & jnp.logical_not(inside))
        def _():
            departures(r, n_head).wait_send()

        def returned_all(count):
            return pltpu.make_async_remote_copy(
                src_ref=o_stage.at[r, pl.ds(0, count)],
                dst_ref=o_stage.at[r, pl.ds(0, count)],
                send_sem=o_send.at[r],
                recv_sem=o_recv.at[r],
                device_id={"kv": jnp.int32(0)},
                device_id_type=MESH,
            )

        @pl.when(inside & (me <= LAST[r]))
        def _():
            returned_all(LAST[r]).wait_send()

        if any(p > LAST[r] for p in PLACE[r]):

            @pl.when(inside & (me > LAST[r]))
            def _():
                returned_all(LAST[r] + 1).wait_send()

        @pl.when(me <= LAST[r])
        def _():
            blocks = x_buf.at[r, pl.ds(0, 2 + 1 + n_tp // 2)]
            pltpu.make_async_remote_copy(
                src_ref=blocks,
                dst_ref=blocks,
                send_sem=g_send.at[r],
                recv_sem=g_recv.at[r, 0],
                device_id={"tp": partner},
                device_id_type=MESH,
            ).wait_send()
            columns_all(r).wait_send()


def body(tokens, lengths, chosen, w_query, w_key, w_value, w_gate, pool_weights, w_out):
    rows, n_seq, depth = tokens.shape
    n_head = w_query.shape[1] // HD
    n_kv, n_tp = lax.axis_size("kv"), lax.axis_size("tp")
    gate_rows = jnp.transpose(w_gate, (1, 2, 0))
    width = w_out.shape[1]
    total = rows * n_seq
    vmem = pl.BlockSpec(memory_space=pltpu.VMEM)
    hbm = pl.BlockSpec(memory_space=pl.ANY)
    dma = pltpu.SemaphoreType.DMA
    full = n_kv * rows

    def whole(*refs):
        kernel(n_kv, n_tp, n_seq, n_head, *refs)

    return pl.pallas_call(
        whole,
        out_shape=jax.ShapeDtypeStruct((rows // n_tp, n_seq, n_tp * width), BF),
        in_specs=[hbm] * 9,
        out_specs=vmem,
        scratch_shapes=[
            pltpu.VMEM((rows, n_seq, depth), BF),
            pltpu.VMEM((total, depth), BF),
            pltpu.VMEM((3, depth, n_head * HD), BF),
            pltpu.VMEM(gate_rows.shape, BF),
            pltpu.VMEM(pool_weights.shape, F32),
            pltpu.VMEM(w_out.shape, BF),
            pltpu.SMEM(lengths.shape, jnp.int32),
            pltpu.SMEM(chosen.shape, jnp.int32),
            pltpu.VMEM((total, total), BF),
            pltpu.VMEM((n_seq * n_head, MSG, rows), BF),
            pltpu.VMEM((n_seq, n_kv, MSG, rows), BF),
            pltpu.VMEM((128, full), BF),
            pltpu.VMEM((128, full), BF),
            pltpu.VMEM((128, full), BF),
            pltpu.VMEM((2 * HD, rows), F32),
            pltpu.VMEM((2 * HD, rows), F32),
            pltpu.VMEM((n_seq, n_kv, HD, rows), BF),
            pltpu.VMEM((n_seq, n_head, HD, rows), BF),
            pltpu.VMEM((n_seq, n_tp, rows, n_head * HD), BF),
            pltpu.VMEM((n_seq, rows, width), BF),
            pltpu.VMEM((n_seq, rows // n_tp, n_tp * width), BF),
            dma((9,)),
            dma((n_seq,)),
            dma((FIRST[-1] + LAST[-1] + 1,)),
            dma((n_seq,)),
            dma((n_seq,)),
            dma((n_seq,)),
            dma((n_seq, 6)),
            dma((n_seq,)),
            dma((n_seq,)),
            pltpu.SemaphoreType.REGULAR((n_kv,)),
            pltpu.SemaphoreType.REGULAR((n_tp,)),
        ],
        compiler_params=pltpu.CompilerParams(
            collective_id=0, has_side_effects=True, vmem_limit_bytes=60 * 2**20
        ),
    )(tokens, lengths, chosen, w_query, w_key, w_value, gate_rows, pool_weights, w_out)


def solution(mesh):
    placed = (
        P("kv", "grp", None),
        P("grp"),
        P("grp", "tp", "kv", None),
        P(None, "tp"),
        P(None, "tp"),
        P(None, "tp"),
        P(None, None, "tp"),
        P(),
        P(None, "tp"),
    )
    return jax.shard_map(
        body, mesh=mesh, in_specs=placed, out_specs=P(("kv", "tp"), "grp", None), check_vma=False
    )
```

```python
import jax
import jax.numpy as jnp
from jax import lax
from jax.experimental import pallas as pl
from jax.experimental.pallas import tpu as pltpu
from jax.sharding import PartitionSpec as P

HD = 64
QB = 64
L_CMP = 32
NEG = -1e30
BF = jnp.bfloat16
F32 = jnp.float32
MESH = pl.DeviceIdType.MESH

ROWS = 128
AUX = 16
MSG = 3 * HD + AUX
KEYS, VALS, QUER, EXTRA = 0, HD, 2 * HD, 3 * HD
LAST = (15, 11, 7, 5)
PLACE = (
    (9, 11, 12, 13),
    (4, 5, 6, 7),
    (3, 4, 1, 2),
    (2, 3, 1, 5),
)
RANK_ORDER = (3, 2, 1, 0)
TILE = 256
AHEAD = 4
MIDDLE = (4, 5)
NEAR = 8
RELAY_SEM = (0, 1, 2, 3, 4, 4, 5, 5, 5, 5)
SHARDS = LAST[0] + 1
PAIRED = sorted({p for places in PLACE for p in places})


def returns_to(i, j):
    return any(i in PLACE[r] and j <= LAST[r] for r in range(len(PLACE)))


def sends_to(i, j):
    asked = any(j in PLACE[r] and i <= LAST[r] for r in range(len(PLACE)))
    return asked or returns_to(i, j)


FIRST = [sum(LAST[:r]) + r for r in range(len(LAST))]


def any_of(me, places):
    here = me < 0
    for p in places:
        here = here | (me == p)
    return here


def iota(shape, dim):
    return lax.broadcasted_iota(jnp.int32, shape, dim)


def nt(a, b):
    return lax.dot_general(a, b, (((1,), (1,)), ((), ())), preferred_element_type=F32)


def nn(a, b):
    return jnp.dot(a, b, preferred_element_type=F32)


def kernel(
    n_kv, n_tp, n_seq, n_head,
    tok_hbm, len_hbm, chosen_hbm, wq_hbm, wk_hbm, wv_hbm, wg_hbm, pw_hbm, wo_hbm,
    out_ref,
    tok, flat, w_buf, wg, pw_ref, wo, len_ref, chosen_ref,
    sel_t, send, recv, k_ext, q_ext, v_all, weight, pool_sum, o_stage, a_buf, x_buf, y_buf, o_buf,
    load_sem, q_send, q_recv, o_send, o_recv, g_send, g_recv, y_send, y_recv,
    ready_kv, ready_tp,
):
    me = lax.axis_index("kv")
    tp = lax.axis_index("tp")
    chips = n_tp // 2
    core = lax.rem(tp, 2)
    chip = tp // 2
    right = lax.rem(chip + 1, chips) * 2 + core
    left = lax.rem(chip + chips - 1, chips) * 2 + core
    far = lax.rem(chip + 2, chips) * 2 + core
    partner = chip * 2 + 1 - core

    barrier = pltpu.get_barrier_semaphore()
    for j in range(n_kv):

        if j == 0:
            tells = (me > 0) & (me < NEAR)
        elif j < NEAR:
            tells = (me > 0) & (me < j)
        else:
            tells = me < j

        @pl.when(tells)
        def _():
            pl.semaphore_signal(
                barrier, inc=1, device_id={"kv": jnp.int32(j)}, device_id_type=MESH
            )

    for t in range(n_tp):

        @pl.when(tp > t)
        def _():
            pl.semaphore_signal(
                barrier, inc=1, device_id={"tp": jnp.int32(t)}, device_id_type=MESH
            )

    loads = [
        pltpu.make_async_copy(len_hbm, len_ref, load_sem.at[0]),
        pltpu.make_async_copy(tok_hbm, tok, load_sem.at[1]),
        pltpu.make_async_copy(wk_hbm, w_buf.at[0], load_sem.at[2]),
        pltpu.make_async_copy(wv_hbm, w_buf.at[1], load_sem.at[3]),
        pltpu.make_async_copy(wq_hbm, w_buf.at[2], load_sem.at[4]),
        pltpu.make_async_copy(wg_hbm, wg, load_sem.at[5]),
        pltpu.make_async_copy(chosen_hbm, chosen_ref, load_sem.at[6]),
        pltpu.make_async_copy(pw_hbm, pw_ref, load_sem.at[7]),
        pltpu.make_async_copy(wo_hbm, wo, load_sem.at[8]),
    ]
    for copy in loads:
        copy.start()
    near = (me > 0) & (me < NEAR)
    told = me + n_tp - 1 - tp - near.astype(jnp.int32) + (me == 0).astype(jnp.int32) * (NEAR - 1)

    def enter():
        @pl.when(told > 0)
        def _():
            pl.semaphore_wait(barrier, told)

        for i in range(n_kv):
            first = NEAR if i == 0 else i + 1
            later = [j for j in range(first, n_kv) if sends_to(i, j)]

            @pl.when(any_of(me, later))
            def _():
                pl.semaphore_signal(
                    ready_kv.at[me], inc=1, device_id={"kv": jnp.int32(i)}, device_id_type=MESH
                )

        for t in range(n_tp):

            @pl.when(tp < t)
            def _():
                pl.semaphore_signal(
                    ready_tp.at[tp], inc=1, device_id={"tp": jnp.int32(t)}, device_id_type=MESH
                )

    pl.when(me > 0)(enter)
    loads[0].wait()

    lens = [len_ref[s] for s in range(n_seq)]
    ranks = []
    for s in range(n_seq):
        rank = jnp.int32(0)
        for o in range(n_seq):
            if o != s:
                ahead = (lens[o] >= lens[s]) if o < s else (lens[o] > lens[s])
                rank = rank + ahead.astype(jnp.int32)
        ranks.append(rank)
    seq_of, len_of = [], []
    for r in range(n_seq):
        seq, length = jnp.int32(0), jnp.int32(0)
        for s in range(n_seq):
            hit = (ranks[s] == r).astype(jnp.int32)
            seq = seq + hit * s
            length = length + hit * lens[s]
        seq_of.append(seq)
        len_of.append(length)

    total = ROWS * n_seq
    row = iota((total, ROWS), 0)
    col = iota((total, ROWS), 1)
    for r in range(n_seq):
        hit = row == col * n_seq + seq_of[r]
        sel_t[:, r * ROWS : (r + 1) * ROWS] = jnp.where(hit, 1.0, 0.0).astype(BF)

    loads[1].wait()
    flat[...] = tok[...].reshape(flat.shape)

    def project(slot, base):
        loads[2 + slot].wait()
        made = nn(flat[...], w_buf[slot]).astype(BF).T
        placed = nn(made, sel_t[...])
        if base == QUER:
            placed = placed * HD**-0.5
        placed = placed.astype(BF)
        for r in range(n_seq):
            for h in range(n_head):
                send[r * n_head + h, base : base + HD, :] = placed[
                    h * HD : (h + 1) * HD, r * ROWS : (r + 1) * ROWS
                ]

    def extras():
        loads[5].wait()
        loads[6].wait()
        gates = jax.nn.sigmoid(nt(wg[...].reshape(2 * n_head, wg.shape[2]), flat[...]))
        gate_hi = gates.astype(BF)
        gate_lo = (gates - gate_hi.astype(F32)).astype(BF)
        gate_rows = nn(jnp.concatenate([gate_hi, gate_lo], axis=0), sel_t[...])
        n_blk, top = chosen_ref.shape[2:]
        slot = iota((top, ROWS), 0)
        blk = iota((top, ROWS), 1) // (ROWS // n_blk)
        for r in range(n_seq):
            cols = slice(r * ROWS, (r + 1) * ROWS)
            for h in range(n_head):
                picked = jnp.zeros((top, ROWS), jnp.int32)
                for b in range(n_blk):
                    for t in range(top):
                        at = (slot == t) & (blk == b)
                        picked = jnp.where(at, chosen_ref[seq_of[r], h, b, t], picked)
                kinds = [
                    gate_rows[g * n_head + h : g * n_head + h + 1, cols] for g in range(4)
                ]
                rest = jnp.zeros((AUX - top - 4, ROWS), F32)
                aux = jnp.concatenate([*kinds, rest, picked.astype(F32)], axis=0)
                send[r * n_head + h, EXTRA:, :] = aux.astype(BF)

    wholes = ((0, MSG),)
    halves = ((0, QUER), (QUER, MSG - QUER))
    thirds = ((KEYS, HD), (VALS, HD), (QUER, MSG - QUER))
    parts_of = {3: thirds, 2: thirds, 1: halves, 0: wholes}

    def message(r, h, part):
        rows = pl.ds(*parts_of[r][part])
        return pltpu.make_async_remote_copy(
            src_ref=send.at[r * n_head + h, rows],
            dst_ref=recv.at[r, me, rows],
            send_sem=q_send.at[r],
            recv_sem=q_recv.at[FIRST[r] + me],
            device_id={"kv": jnp.int32(PLACE[r][h])},
            device_id_type=MESH,
        )

    def arrival(r, j):
        return pltpu.make_async_remote_copy(
            src_ref=send.at[0],
            dst_ref=recv.at[r, j],
            send_sem=q_send.at[r],
            recv_sem=q_recv.at[FIRST[r] + j],
            device_id={"kv": jnp.int32(0)},
            device_id_type=MESH,
        )

    def departures(r, count):
        return pltpu.make_async_remote_copy(
            src_ref=send.at[pl.ds(0, count)],
            dst_ref=send.at[pl.ds(0, count)],
            send_sem=q_send.at[r],
            recv_sem=q_recv.at[0],
            device_id={"kv": jnp.int32(0)},
            device_id_type=MESH,
        )

    def await_ready(there):
        first = 1 if there < NEAR else 0

        @pl.when(any_of(me, [i for i in range(first, there) if sends_to(i, there)]))
        def _():
            pl.semaphore_wait(ready_kv.at[there], 1)

    asked = set()

    def send_rank(r, part):
        for h in sorted(range(n_head), key=lambda h: PLACE[r][h]):
            there = PLACE[r][h]
            if there not in asked:
                asked.add(there)
                await_ready(there)

            @pl.when((me <= LAST[r]) & (me != there))
            def _():
                message(r, h, part).start()

    ahead = me < AHEAD
    early = (me > 0) & ahead
    project(0, KEYS)

    @pl.when(jnp.logical_not(ahead))
    def _():
        send_rank(3, 0)
        send_rank(2, 0)

    project(1, VALS)

    def send_to(there, wanted):
        for r in (3, 2, 1, 0):
            for h in range(n_head):
                if PLACE[r][h] == there:
                    for part in wanted(r):

                        @pl.when(me != there)
                        def _():
                            message(r, h, part).start()

    @pl.when(jnp.logical_not(ahead))
    def _():
        send_rank(3, 1)
        send_rank(2, 1)

    def but_last(r):
        return range(len(parts_of[r]) - 1)

    def only_last(r):
        return [len(parts_of[r]) - 1]

    def every(r):
        return range(len(parts_of[r]))

    near_by = [p for p in PAIRED if p < MIDDLE[0]]
    beyond = [p for p in PAIRED if p > MIDDLE[-1]]

    @pl.when(early)
    def _():
        for there in near_by:
            await_ready(there)
            send_to(there, but_last)

    project(2, QUER)

    @pl.when(jnp.logical_not(ahead))
    def _():
        send_rank(1, 0)

    @pl.when(early)
    def _():
        for there in MIDDLE:
            await_ready(there)
            send_to(there, but_last)

    extras()
    for r in range(n_seq):
        for h in range(n_head):
            there = PLACE[r][h]
            if there <= LAST[r]:

                @pl.when(me == there)
                def _():
                    recv[r, there] = send[r * n_head + h]

    @pl.when(early)
    def _():
        for there in (*near_by, *MIDDLE):
            send_to(there, only_last)
        for there in beyond:
            await_ready(there)
            send_to(there, every)

    @pl.when(me == 0)
    def _():
        enter()
        for there in [p for p in PAIRED if MIDDLE[0] <= p < NEAR] + near_by:
            send_to(there, every)
        for there in beyond:
            if there >= NEAR:
                await_ready(there)
                send_to(there, every)

    @pl.when(jnp.logical_not(ahead))
    def _():
        send_rank(3, 2)
        send_rank(2, 2)
        send_rank(1, 1)
        send_rank(0, 0)

    loads[7].wait()

    def returned(r, h_here, j):
        return pltpu.make_async_remote_copy(
            src_ref=o_stage.at[r, j],
            dst_ref=a_buf.at[r, h_here],
            send_sem=o_send.at[r],
            recv_sem=o_recv.at[r],
            device_id={"kv": jnp.int32(j)},
            device_id_type=MESH,
        )

    def attend(r):
        shards = LAST[r] + 1
        span = shards * ROWS
        length = len_of[r]
        head = jnp.int32(0)
        for h in range(n_head):
            head = head + (me == PLACE[r][h]).astype(jnp.int32) * h

        pw_keys = jnp.concatenate([pw_ref[0].T] * (ROWS // L_CMP), axis=1)
        pw_vals = jnp.concatenate([pw_ref[1].T] * (ROWS // L_CMP), axis=1)
        weight[...] = jnp.concatenate([pw_keys, pw_vals], axis=0)
        lane_blk = iota((ROWS, ROWS), 0) // L_CMP
        lane_col = iota((ROWS, ROWS), 1)

        def prepare(j):
            @pl.when(me != j)
            def _():
                arrival(r, j).wait_recv()

            cols = slice(j * ROWS, (j + 1) * ROWS)
            q_ext[0:HD, cols] = recv[r, j, QUER:EXTRA, :]
            k_ext[0:HD, cols] = recv[r, j, KEYS:VALS, :]
            v_all[0:HD, cols] = recv[r, j, VALS:QUER, :]
            picks = recv[r, j, EXTRA:MSG, :].astype(F32)
            blocks = iota((32, ROWS), 0).astype(F32)
            hit = blocks == picks[8:9]
            for t in range(1, 8):
                hit = hit | (blocks == picks[8 + t : 9 + t])
            q_ext[HD : HD + 32, cols] = jnp.where(hit, 0.0, NEG).astype(BF)
            one_row = (iota((32, ROWS), 0) == 0).astype(F32)
            q_ext[HD + 32 :, cols] = one_row.astype(BF)
            key = j * ROWS + iota((32, ROWS), 1)
            k_ext[HD : HD + 32, cols] = (iota((32, ROWS), 0) == key // QB).astype(F32).astype(BF)
            k_ext[HD + 32 :, cols] = jnp.where(key >= length, one_row * NEG, 0.0).astype(BF)
            v_all[HD:, cols] = (iota((HD, ROWS), 0) == 0).astype(F32).astype(BF)
            prod = recv[r, j, KEYS:QUER, :].astype(F32) * weight[...]
            hi = prod.astype(BF)
            lo = (prod - hi.astype(F32)).astype(BF)
            group = jnp.where(lane_col == j * (ROWS // L_CMP) + lane_blk, 1.0, 0.0).astype(BF)
            return [hi, lo], [group, group]

        pool_sum[...] = jnp.zeros((2 * HD, ROWS), F32)
        for t in range(span // TILE):
            lo, hi = t * TILE, (t + 1) * TILE
            lefts, rights = [], []
            for i in range(TILE // ROWS):
                left_i, right_i = prepare(t * (TILE // ROWS) + i)
                lefts, rights = lefts + left_i, rights + right_i
            fresh = nn(jnp.concatenate(lefts, axis=1), jnp.concatenate(rights, axis=0))
            known = lane_col < t * (TILE // L_CMP)
            pool_sum[...] = jnp.where(known, pool_sum[...], fresh)
            pooled = pool_sum[...].astype(BF)
            key_pooled = jnp.concatenate([pooled[:HD], jnp.zeros((HD, ROWS), BF)], axis=0)
            val_pooled = pooled[HD:]
            q = q_ext[:, lo:hi].T
            scores = nn(q, k_ext[:, :hi])
            edge = jnp.where(
                iota((TILE, TILE), 1) <= iota((TILE, TILE), 0), scores[:, lo:hi], NEG
            )
            scores = edge if t == 0 else jnp.concatenate([scores[:, :lo], edge], axis=1)
            top = jnp.max(scores, axis=1, keepdims=True)
            e = jnp.exp(scores - top)
            summed = nt(e.astype(BF), v_all[:, :hi])
            picked_out = summed[:, :HD] / summed[:, HD : HD + 1]

            scores = nn(q, key_pooled)
            pos = lo + iota((TILE, ROWS), 0)
            end = iota((TILE, ROWS), 1) * L_CMP + (L_CMP - 1)
            usable = (end <= pos) & (end < length)
            top = jnp.max(jnp.where(usable, scores, NEG), axis=1, keepdims=True)
            e = jnp.where(usable, jnp.exp(jnp.where(usable, scores, NEG) - top), 0.0)
            tot = jnp.sum(e, axis=1, keepdims=True)
            pooled_out = nt(e.astype(BF), val_pooled) / jnp.where(tot > 0, tot, 1.0)

            both = jnp.concatenate([pooled_out, picked_out], axis=1).T
            for i in range(TILE // ROWS):
                j = t * (TILE // ROWS) + i
                g = recv[r, j, EXTRA:MSG, :].astype(F32)
                part = both[:, i * ROWS : (i + 1) * ROWS]
                mix = (g[0:1] + g[2:3]) * part[:HD] + (g[1:2] + g[3:4]) * part[HD:]
                alive = j * ROWS + iota((HD, ROWS), 1) < length
                o_stage[r, j] = jnp.where(alive, mix, 0.0).astype(BF)

                if j not in PAIRED:
                    before = RANK_ORDER[: RANK_ORDER.index(r)]
                    new = [
                        p
                        for p in PLACE[r]
                        if p < j and not any(p in PLACE[q] and j <= LAST[q] for q in before)
                    ]

                    @pl.when(any_of(me, new))
                    def _():
                        pl.semaphore_wait(ready_kv.at[j], 1)

                @pl.when(me != j)
                def _():
                    returned(r, head, j).start()

                @pl.when(me == j)
                def _():
                    a_buf[r, head] = o_stage[r, j]

    for r in RANK_ORDER:

        @pl.when(any_of(me, PLACE[r]))
        def _():
            attend(r)

    half = ROWS // 2
    lower, upper = pl.ds(0, half), pl.ds(half, half)

    def hop(r, block, rows, to, n):
        ref = x_buf.at[r, block] if rows is None else x_buf.at[r, block, rows]
        return pltpu.make_async_remote_copy(
            src_ref=ref,
            dst_ref=ref,
            send_sem=g_send.at[r],
            recv_sem=g_recv.at[r, RELAY_SEM[n]],
            device_id={"tp": to},
            device_id_type=MESH,
        )

    def sent(r, n):
        return hop(r, *(
            (tp, lower, right, 0),
            (tp, upper, right, 1),
            (tp, upper, left, 2),
            (tp, lower, left, 3),
            (left, lower, right, 4),
            (right, upper, left, 5),
            (tp, None, partner, 6),
            (left, None, partner, 7),
            (right, None, partner, 8),
            (far, None, partner, 9),
        )[n])

    def other(t):
        return t + 1 - 2 * lax.rem(t, 2)

    def received(r, n):
        return hop(r, *(
            (left, lower, left, 0),
            (left, upper, left, 1),
            (right, upper, right, 2),
            (right, lower, right, 3),
            (far, lower, left, 4),
            (far, upper, right, 5),
            (other(tp), None, partner, 6),
            (other(left), None, partner, 7),
            (other(right), None, partner, 8),
            (other(far), None, partner, 9),
        )[n])

    rows_each = ROWS // n_tp
    width = wo.shape[1]

    def column_copy(r, to):
        return pltpu.make_async_remote_copy(
            src_ref=y_buf.at[r, pl.ds(pl.multiple_of(to * rows_each, rows_each), rows_each)],
            dst_ref=o_buf.at[r, :, pl.ds(pl.multiple_of(tp * width, width), width)],
            send_sem=y_send.at[r],
            recv_sem=y_recv.at[r],
            device_id={"tp": to},
            device_id_type=MESH,
        )

    def columns_all(r):
        rest = pl.ds(0, (n_tp - 1) * rows_each)
        return pltpu.make_async_remote_copy(
            src_ref=y_buf.at[r, rest],
            dst_ref=y_buf.at[r, rest],
            send_sem=y_send.at[r],
            recv_sem=y_recv.at[r],
            device_id={"tp": partner},
            device_id_type=MESH,
        )

    loads[8].wait()
    for t in range(n_tp):

        @pl.when(tp > t)
        def _():
            pl.semaphore_wait(ready_tp.at[t], 1)


    def handed_back(r, count):
        return pltpu.make_async_remote_copy(
            src_ref=o_stage.at[r, pl.ds(0, count)],
            dst_ref=a_buf.at[r, pl.ds(0, count)],
            send_sem=o_send.at[r],
            recv_sem=o_recv.at[r],
            device_id={"kv": jnp.int32(0)},
            device_id_type=MESH,
        )

    def own(r):
        inside = any_of(me, PLACE[r])

        @pl.when(inside)
        def _():
            handed_back(r, n_head - 1).wait_recv()

        @pl.when(jnp.logical_not(inside))
        def _():
            handed_back(r, n_head).wait_recv()

        x_buf[r, tp] = a_buf[r].reshape(n_head * HD, ROWS).T
        for n in (0, 2, 1, 3, 6):
            sent(r, n).start()

    def relay(r):
        received(r, 0).wait_recv()
        sent(r, 4).start()
        received(r, 2).wait_recv()
        sent(r, 5).start()
        received(r, 1).wait_recv()
        sent(r, 7).start()
        received(r, 3).wait_recv()
        sent(r, 8).start()

    def across(r):
        hop(r, far, None, left, 4).wait_recv()
        sent(r, 9).start()

    def mix(r):
        blocks = x_buf.at[r, pl.ds(0, n_tp // 2)]
        pltpu.make_async_remote_copy(
            src_ref=blocks,
            dst_ref=blocks,
            send_sem=g_send.at[r],
            recv_sem=g_recv.at[r, RELAY_SEM[6]],
            device_id={"tp": partner},
            device_id_type=MESH,
        ).wait_recv()
        rows = jnp.concatenate([x_buf[r, g] for g in range(n_tp)], axis=1)
        y_buf[r] = nn(rows, wo[...]).astype(BF)
        for step in range(1, n_tp):
            column_copy(r, lax.rem(tp + step, n_tp)).start()
        mine = pl.ds(pl.multiple_of(tp * rows_each, rows_each), rows_each)
        o_buf[r, :, pl.ds(pl.multiple_of(tp * width, width), width)] = y_buf[r, mine]

    def stage(step, r):
        @pl.when(me <= LAST[r])
        def _():
            step(r)

    first, second, third, last = RANK_ORDER
    for step, r in (
        (own, first), (own, second), (relay, first), (own, third), (relay, second), (own, last),
        (across, first), (relay, third), (across, second), (mix, first), (relay, last),
        (across, third), (mix, second), (across, last), (mix, third), (mix, last),
    ):
        stage(step, r)

    for r in range(n_seq):

        @pl.when(me > LAST[r])
        def _():
            o_buf[r] = jnp.zeros(o_buf.shape[1:], BF)

    for r in range(n_seq):

        @pl.when(me <= LAST[r])
        def _():
            columns_all(r).wait_recv()

    many = rows_each * n_seq
    want = iota((many, many), 0)
    have = iota((many, many), 1)
    pick = jnp.zeros((many, many), F32)
    for r in range(n_seq):
        hit = (have == r * rows_each + want // n_seq) & (lax.rem(want, n_seq) == seq_of[r])
        pick = jnp.where(hit, 1.0, pick)
    pick = pick.astype(BF)
    for c in range(n_tp):
        cols = slice(c * width, (c + 1) * width)
        rows = o_buf[:, :, cols].reshape(many, width)
        out_ref[:, :, cols] = nn(pick, rows).astype(BF).reshape(rows_each, n_seq, width)

    for r in range(n_seq):
        inside = any_of(me, PLACE[r])

        @pl.when((me <= LAST[r]) & inside)
        def _():
            departures(r, n_head - 1).wait_send()

        @pl.when((me <= LAST[r]) & jnp.logical_not(inside))
        def _():
            departures(r, n_head).wait_send()

        def returned_all(count):
            return pltpu.make_async_remote_copy(
                src_ref=o_stage.at[r, pl.ds(0, count)],
                dst_ref=o_stage.at[r, pl.ds(0, count)],
                send_sem=o_send.at[r],
                recv_sem=o_recv.at[r],
                device_id={"kv": jnp.int32(0)},
                device_id_type=MESH,
            )

        @pl.when(inside & (me <= LAST[r]))
        def _():
            returned_all(LAST[r]).wait_send()

        if any(p > LAST[r] for p in PLACE[r]):

            @pl.when(inside & (me > LAST[r]))
            def _():
                returned_all(LAST[r] + 1).wait_send()

        @pl.when(me <= LAST[r])
        def _():
            blocks = x_buf.at[r, pl.ds(0, 2 + 1 + n_tp // 2)]
            pltpu.make_async_remote_copy(
                src_ref=blocks,
                dst_ref=blocks,
                send_sem=g_send.at[r],
                recv_sem=g_recv.at[r, 0],
                device_id={"tp": partner},
                device_id_type=MESH,
            ).wait_send()
            columns_all(r).wait_send()


def body(tokens, lengths, chosen, w_query, w_key, w_value, w_gate, pool_weights, w_out):
    rows, n_seq, depth = tokens.shape
    n_head = w_query.shape[1] // HD
    n_kv, n_tp = lax.axis_size("kv"), lax.axis_size("tp")
    gate_rows = jnp.transpose(w_gate, (1, 2, 0))
    width = w_out.shape[1]
    total = rows * n_seq
    vmem = pl.BlockSpec(memory_space=pltpu.VMEM)
    hbm = pl.BlockSpec(memory_space=pl.ANY)
    dma = pltpu.SemaphoreType.DMA
    full = n_kv * rows

    def whole(*refs):
        kernel(n_kv, n_tp, n_seq, n_head, *refs)

    return pl.pallas_call(
        whole,
        out_shape=jax.ShapeDtypeStruct((rows // n_tp, n_seq, n_tp * width), BF),
        in_specs=[hbm] * 9,
        out_specs=vmem,
        scratch_shapes=[
            pltpu.VMEM((rows, n_seq, depth), BF),
            pltpu.VMEM((total, depth), BF),
            pltpu.VMEM((3, depth, n_head * HD), BF),
            pltpu.VMEM(gate_rows.shape, BF),
            pltpu.VMEM(pool_weights.shape, F32),
            pltpu.VMEM(w_out.shape, BF),
            pltpu.SMEM(lengths.shape, jnp.int32),
            pltpu.SMEM(chosen.shape, jnp.int32),
            pltpu.VMEM((total, total), BF),
            pltpu.VMEM((n_seq * n_head, MSG, rows), BF),
            pltpu.VMEM((n_seq, n_kv, MSG, rows), BF),
            pltpu.VMEM((128, full), BF),
            pltpu.VMEM((128, full), BF),
            pltpu.VMEM((128, full), BF),
            pltpu.VMEM((2 * HD, rows), F32),
            pltpu.VMEM((2 * HD, rows), F32),
            pltpu.VMEM((n_seq, n_kv, HD, rows), BF),
            pltpu.VMEM((n_seq, n_head, HD, rows), BF),
            pltpu.VMEM((n_seq, n_tp, rows, n_head * HD), BF),
            pltpu.VMEM((n_seq, rows, width), BF),
            pltpu.VMEM((n_seq, rows // n_tp, n_tp * width), BF),
            dma((9,)),
            dma((n_seq,)),
            dma((FIRST[-1] + LAST[-1] + 1,)),
            dma((n_seq,)),
            dma((n_seq,)),
            dma((n_seq,)),
            dma((n_seq, 6)),
            dma((n_seq,)),
            dma((n_seq,)),
            pltpu.SemaphoreType.REGULAR((n_kv,)),
            pltpu.SemaphoreType.REGULAR((n_tp,)),
        ],
        compiler_params=pltpu.CompilerParams(
            collective_id=0, has_side_effects=True, vmem_limit_bytes=60 * 2**20
        ),
    )(tokens, lengths, chosen, w_query, w_key, w_value, gate_rows, pool_weights, w_out)


def solution(mesh):
    placed = (
        P("kv", "grp", None),
        P("grp"),
        P("grp", "tp", "kv", None),
        P(None, "tp"),
        P(None, "tp"),
        P(None, "tp"),
        P(None, None, "tp"),
        P(),
        P(None, "tp"),
    )
    return jax.shard_map(
        body, mesh=mesh, in_specs=placed, out_specs=P(("kv", "tp"), "grp", None), check_vma=False
    )
```

```python
import jax
import jax.numpy as jnp
from jax import lax
from jax.experimental import pallas as pl
from jax.experimental.pallas import tpu as pltpu
from jax.sharding import PartitionSpec as P

HD = 64
QB = 64
L_CMP = 32
NEG = -1e30
BF = jnp.bfloat16
F32 = jnp.float32
MESH = pl.DeviceIdType.MESH

ROWS = 128
AUX = 16
MSG = 3 * HD + AUX
KEYS, VALS, QUER, EXTRA = 0, HD, 2 * HD, 3 * HD
LAST = (15, 11, 7, 5)
PLACE = (
    (9, 11, 12, 13),
    (4, 5, 6, 7),
    (3, 4, 1, 2),
    (2, 3, 1, 5),
)
RANK_ORDER = (1, 2, 3, 0)
TILE = 256
AHEAD = 4
MIDDLE = (4, 5)
NEAR = 8
RELAY_SEM = (0, 1, 2, 3, 4, 4, 5, 5, 5, 5)
SHARDS = LAST[0] + 1
PAIRED = sorted({p for places in PLACE for p in places})


def returns_to(i, j):
    return any(i in PLACE[r] and j <= LAST[r] for r in range(len(PLACE)))


def sends_to(i, j):
    asked = any(j in PLACE[r] and i <= LAST[r] for r in range(len(PLACE)))
    return asked or returns_to(i, j)


FIRST = [sum(LAST[:r]) + r for r in range(len(LAST))]


def any_of(me, places):
    here = me < 0
    for p in places:
        here = here | (me == p)
    return here


def iota(shape, dim):
    return lax.broadcasted_iota(jnp.int32, shape, dim)


def nt(a, b):
    return lax.dot_general(a, b, (((1,), (1,)), ((), ())), preferred_element_type=F32)


def nn(a, b):
    return jnp.dot(a, b, preferred_element_type=F32)


def kernel(
    n_kv, n_tp, n_seq, n_head,
    tok_hbm, len_hbm, chosen_hbm, wq_hbm, wk_hbm, wv_hbm, wg_hbm, pw_hbm, wo_hbm,
    out_ref,
    tok, flat, w_buf, wg, pw_ref, wo, len_ref, chosen_ref,
    sel_t, send, recv, k_ext, q_ext, v_all, weight, pool_sum, o_stage, a_buf, x_buf, y_buf, o_buf,
    load_sem, q_send, q_recv, o_send, o_recv, g_send, g_recv, y_send, y_recv,
    ready_kv, ready_tp,
):
    me = lax.axis_index("kv")
    tp = lax.axis_index("tp")
    chips = n_tp // 2
    core = lax.rem(tp, 2)
    chip = tp // 2
    right = lax.rem(chip + 1, chips) * 2 + core
    left = lax.rem(chip + chips - 1, chips) * 2 + core
    far = lax.rem(chip + 2, chips) * 2 + core
    partner = chip * 2 + 1 - core

    barrier = pltpu.get_barrier_semaphore()
    for j in range(n_kv):

        if j == 0:
            tells = (me > 0) & (me < NEAR)
        elif j < NEAR:
            tells = (me > 0) & (me < j)
        else:
            tells = me < j

        @pl.when(tells)
        def _():
            pl.semaphore_signal(
                barrier, inc=1, device_id={"kv": jnp.int32(j)}, device_id_type=MESH
            )

    for t in range(n_tp):

        @pl.when(tp > t)
        def _():
            pl.semaphore_signal(
                barrier, inc=1, device_id={"tp": jnp.int32(t)}, device_id_type=MESH
            )

    loads = [
        pltpu.make_async_copy(len_hbm, len_ref, load_sem.at[0]),
        pltpu.make_async_copy(tok_hbm, tok, load_sem.at[1]),
        pltpu.make_async_copy(wk_hbm, w_buf.at[0], load_sem.at[2]),
        pltpu.make_async_copy(wv_hbm, w_buf.at[1], load_sem.at[3]),
        pltpu.make_async_copy(wq_hbm, w_buf.at[2], load_sem.at[4]),
        pltpu.make_async_copy(wg_hbm, wg, load_sem.at[5]),
        pltpu.make_async_copy(chosen_hbm, chosen_ref, load_sem.at[6]),
        pltpu.make_async_copy(pw_hbm, pw_ref, load_sem.at[7]),
        pltpu.make_async_copy(wo_hbm, wo, load_sem.at[8]),
    ]
    for copy in loads:
        copy.start()
    near = (me > 0) & (me < NEAR)
    told = me + n_tp - 1 - tp - near.astype(jnp.int32) + (me == 0).astype(jnp.int32) * (NEAR - 1)

    def enter():
        @pl.when(told > 0)
        def _():
            pl.semaphore_wait(barrier, told)

        for i in range(n_kv):
            first = NEAR if i == 0 else i + 1
            later = [j for j in range(first, n_kv) if sends_to(i, j)]

            @pl.when(any_of(me, later))
            def _():
                pl.semaphore_signal(
                    ready_kv.at[me], inc=1, device_id={"kv": jnp.int32(i)}, device_id_type=MESH
                )

        for t in range(n_tp):

            @pl.when(tp < t)
            def _():
                pl.semaphore_signal(
                    ready_tp.at[tp], inc=1, device_id={"tp": jnp.int32(t)}, device_id_type=MESH
                )

    pl.when(me > 0)(enter)
    loads[0].wait()

    lens = [len_ref[s] for s in range(n_seq)]
    ranks = []
    for s in range(n_seq):
        rank = jnp.int32(0)
        for o in range(n_seq):
            if o != s:
                ahead = (lens[o] >= lens[s]) if o < s else (lens[o] > lens[s])
                rank = rank + ahead.astype(jnp.int32)
        ranks.append(rank)
    seq_of, len_of = [], []
    for r in range(n_seq):
        seq, length = jnp.int32(0), jnp.int32(0)
        for s in range(n_seq):
            hit = (ranks[s] == r).astype(jnp.int32)
            seq = seq + hit * s
            length = length + hit * lens[s]
        seq_of.append(seq)
        len_of.append(length)

    total = ROWS * n_seq
    row = iota((total, ROWS), 0)
    col = iota((total, ROWS), 1)
    for r in range(n_seq):
        hit = row == col * n_seq + seq_of[r]
        sel_t[:, r * ROWS : (r + 1) * ROWS] = jnp.where(hit, 1.0, 0.0).astype(BF)

    loads[1].wait()
    flat[...] = tok[...].reshape(flat.shape)

    def project(slot, base):
        loads[2 + slot].wait()
        made = nn(flat[...], w_buf[slot]).astype(BF).T
        placed = nn(made, sel_t[...])
        if base == QUER:
            placed = placed * HD**-0.5
        placed = placed.astype(BF)
        for r in range(n_seq):
            for h in range(n_head):
                send[r * n_head + h, base : base + HD, :] = placed[
                    h * HD : (h + 1) * HD, r * ROWS : (r + 1) * ROWS
                ]

    def extras():
        loads[5].wait()
        loads[6].wait()
        gates = jax.nn.sigmoid(nt(wg[...].reshape(2 * n_head, wg.shape[2]), flat[...]))
        gate_hi = gates.astype(BF)
        gate_lo = (gates - gate_hi.astype(F32)).astype(BF)
        gate_rows = nn(jnp.concatenate([gate_hi, gate_lo], axis=0), sel_t[...])
        n_blk, top = chosen_ref.shape[2:]
        slot = iota((top, ROWS), 0)
        blk = iota((top, ROWS), 1) // (ROWS // n_blk)
        for r in range(n_seq):
            cols = slice(r * ROWS, (r + 1) * ROWS)
            for h in range(n_head):
                picked = jnp.zeros((top, ROWS), jnp.int32)
                for b in range(n_blk):
                    for t in range(top):
                        at = (slot == t) & (blk == b)
                        picked = jnp.where(at, chosen_ref[seq_of[r], h, b, t], picked)
                kinds = [
                    gate_rows[g * n_head + h : g * n_head + h + 1, cols] for g in range(4)
                ]
                rest = jnp.zeros((AUX - top - 4, ROWS), F32)
                aux = jnp.concatenate([*kinds, rest, picked.astype(F32)], axis=0)
                send[r * n_head + h, EXTRA:, :] = aux.astype(BF)

    wholes = ((0, MSG),)
    halves = ((0, QUER), (QUER, MSG - QUER))
    thirds = ((KEYS, HD), (VALS, HD), (QUER, MSG - QUER))
    parts_of = {3: thirds, 2: thirds, 1: halves, 0: wholes}

    def message(r, h, part):
        rows = pl.ds(*parts_of[r][part])
        return pltpu.make_async_remote_copy(
            src_ref=send.at[r * n_head + h, rows],
            dst_ref=recv.at[r, me, rows],
            send_sem=q_send.at[r],
            recv_sem=q_recv.at[FIRST[r] + me],
            device_id={"kv": jnp.int32(PLACE[r][h])},
            device_id_type=MESH,
        )

    def arrival(r, j):
        return pltpu.make_async_remote_copy(
            src_ref=send.at[0],
            dst_ref=recv.at[r, j],
            send_sem=q_send.at[r],
            recv_sem=q_recv.at[FIRST[r] + j],
            device_id={"kv": jnp.int32(0)},
            device_id_type=MESH,
        )

    def departures(r, count):
        return pltpu.make_async_remote_copy(
            src_ref=send.at[pl.ds(0, count)],
            dst_ref=send.at[pl.ds(0, count)],
            send_sem=q_send.at[r],
            recv_sem=q_recv.at[0],
            device_id={"kv": jnp.int32(0)},
            device_id_type=MESH,
        )

    def await_ready(there):
        first = 1 if there < NEAR else 0

        @pl.when(any_of(me, [i for i in range(first, there) if sends_to(i, there)]))
        def _():
            pl.semaphore_wait(ready_kv.at[there], 1)

    asked = set()

    def send_rank(r, part):
        for h in sorted(range(n_head), key=lambda h: PLACE[r][h]):
            there = PLACE[r][h]
            if there not in asked:
                asked.add(there)
                await_ready(there)

            @pl.when((me <= LAST[r]) & (me != there))
            def _():
                message(r, h, part).start()

    ahead = me < AHEAD
    early = (me > 0) & ahead
    project(0, KEYS)

    @pl.when(jnp.logical_not(ahead))
    def _():
        send_rank(3, 0)
        send_rank(2, 0)

    project(1, VALS)

    def send_to(there, wanted):
        for r in (3, 2, 1, 0):
            for h in range(n_head):
                if PLACE[r][h] == there:
                    for part in wanted(r):

                        @pl.when(me != there)
                        def _():
                            message(r, h, part).start()

    @pl.when(jnp.logical_not(ahead))
    def _():
        send_rank(3, 1)
        send_rank(2, 1)

    def but_last(r):
        return range(len(parts_of[r]) - 1)

    def only_last(r):
        return [len(parts_of[r]) - 1]

    def every(r):
        return range(len(parts_of[r]))

    near_by = [p for p in PAIRED if p < MIDDLE[0]]
    beyond = [p for p in PAIRED if p > MIDDLE[-1]]

    @pl.when(early)
    def _():
        for there in near_by:
            await_ready(there)
            send_to(there, but_last)

    project(2, QUER)

    @pl.when(jnp.logical_not(ahead))
    def _():
        send_rank(1, 0)

    @pl.when(early)
    def _():
        for there in MIDDLE:
            await_ready(there)
            send_to(there, but_last)

    extras()
    for r in range(n_seq):
        for h in range(n_head):
            there = PLACE[r][h]
            if there <= LAST[r]:

                @pl.when(me == there)
                def _():
                    recv[r, there] = send[r * n_head + h]

    @pl.when(early)
    def _():
        for there in (*near_by, *MIDDLE):
            send_to(there, only_last)
        for there in beyond:
            await_ready(there)
            send_to(there, every)

    @pl.when(me == 0)
    def _():
        enter()
        for there in [p for p in PAIRED if MIDDLE[0] <= p < NEAR] + near_by:
            send_to(there, every)
        for there in beyond:
            if there >= NEAR:
                await_ready(there)
                send_to(there, every)

    @pl.when(jnp.logical_not(ahead))
    def _():
        send_rank(3, 2)
        send_rank(2, 2)
        send_rank(1, 1)
        send_rank(0, 0)

    loads[7].wait()

    def returned(r, h_here, j):
        return pltpu.make_async_remote_copy(
            src_ref=o_stage.at[r, j],
            dst_ref=a_buf.at[r, h_here],
            send_sem=o_send.at[r],
            recv_sem=o_recv.at[r],
            device_id={"kv": jnp.int32(j)},
            device_id_type=MESH,
        )

    def attend(r):
        shards = LAST[r] + 1
        span = shards * ROWS
        length = len_of[r]
        head = jnp.int32(0)
        for h in range(n_head):
            head = head + (me == PLACE[r][h]).astype(jnp.int32) * h

        pw_keys = jnp.concatenate([pw_ref[0].T] * (ROWS // L_CMP), axis=1)
        pw_vals = jnp.concatenate([pw_ref[1].T] * (ROWS // L_CMP), axis=1)
        weight[...] = jnp.concatenate([pw_keys, pw_vals], axis=0)
        lane_blk = iota((ROWS, ROWS), 0) // L_CMP
        lane_col = iota((ROWS, ROWS), 1)

        def prepare(j):
            @pl.when(me != j)
            def _():
                arrival(r, j).wait_recv()

            cols = slice(j * ROWS, (j + 1) * ROWS)
            q_ext[0:HD, cols] = recv[r, j, QUER:EXTRA, :]
            k_ext[0:HD, cols] = recv[r, j, KEYS:VALS, :]
            v_all[0:HD, cols] = recv[r, j, VALS:QUER, :]
            picks = recv[r, j, EXTRA:MSG, :].astype(F32)
            blocks = iota((32, ROWS), 0).astype(F32)
            hit = blocks == picks[8:9]
            for t in range(1, 8):
                hit = hit | (blocks == picks[8 + t : 9 + t])
            q_ext[HD : HD + 32, cols] = jnp.where(hit, 0.0, NEG).astype(BF)
            one_row = (iota((32, ROWS), 0) == 0).astype(F32)
            q_ext[HD + 32 :, cols] = one_row.astype(BF)
            key = j * ROWS + iota((32, ROWS), 1)
            k_ext[HD : HD + 32, cols] = (iota((32, ROWS), 0) == key // QB).astype(F32).astype(BF)
            k_ext[HD + 32 :, cols] = jnp.where(key >= length, one_row * NEG, 0.0).astype(BF)
            v_all[HD:, cols] = (iota((HD, ROWS), 0) == 0).astype(F32).astype(BF)
            prod = recv[r, j, KEYS:QUER, :].astype(F32) * weight[...]
            hi = prod.astype(BF)
            lo = (prod - hi.astype(F32)).astype(BF)
            group = jnp.where(lane_col == j * (ROWS // L_CMP) + lane_blk, 1.0, 0.0).astype(BF)
            return [hi, lo], [group, group]

        pool_sum[...] = jnp.zeros((2 * HD, ROWS), F32)
        for t in range(span // TILE):
            lo, hi = t * TILE, (t + 1) * TILE
            lefts, rights = [], []
            for i in range(TILE // ROWS):
                left_i, right_i = prepare(t * (TILE // ROWS) + i)
                lefts, rights = lefts + left_i, rights + right_i
            fresh = nn(jnp.concatenate(lefts, axis=1), jnp.concatenate(rights, axis=0))
            known = lane_col < t * (TILE // L_CMP)
            pool_sum[...] = jnp.where(known, pool_sum[...], fresh)
            pooled = pool_sum[...].astype(BF)
            key_pooled = jnp.concatenate([pooled[:HD], jnp.zeros((HD, ROWS), BF)], axis=0)
            val_pooled = pooled[HD:]
            q = q_ext[:, lo:hi].T
            scores = nn(q, k_ext[:, :hi])
            edge = jnp.where(
                iota((TILE, TILE), 1) <= iota((TILE, TILE), 0), scores[:, lo:hi], NEG
            )
            scores = edge if t == 0 else jnp.concatenate([scores[:, :lo], edge], axis=1)
            top = jnp.max(scores, axis=1, keepdims=True)
            e = jnp.exp(scores - top)
            summed = nt(e.astype(BF), v_all[:, :hi])
            picked_out = summed[:, :HD] / summed[:, HD : HD + 1]

            scores = nn(q, key_pooled)
            pos = lo + iota((TILE, ROWS), 0)
            end = iota((TILE, ROWS), 1) * L_CMP + (L_CMP - 1)
            usable = (end <= pos) & (end < length)
            top = jnp.max(jnp.where(usable, scores, NEG), axis=1, keepdims=True)
            e = jnp.where(usable, jnp.exp(jnp.where(usable, scores, NEG) - top), 0.0)
            tot = jnp.sum(e, axis=1, keepdims=True)
            pooled_out = nt(e.astype(BF), val_pooled) / jnp.where(tot > 0, tot, 1.0)

            both = jnp.concatenate([pooled_out, picked_out], axis=1).T
            for i in range(TILE // ROWS):
                j = t * (TILE // ROWS) + i
                g = recv[r, j, EXTRA:MSG, :].astype(F32)
                part = both[:, i * ROWS : (i + 1) * ROWS]
                mix = (g[0:1] + g[2:3]) * part[:HD] + (g[1:2] + g[3:4]) * part[HD:]
                alive = j * ROWS + iota((HD, ROWS), 1) < length
                o_stage[r, j] = jnp.where(alive, mix, 0.0).astype(BF)

                if j not in PAIRED:
                    before = RANK_ORDER[: RANK_ORDER.index(r)]
                    new = [
                        p
                        for p in PLACE[r]
                        if p < j and not any(p in PLACE[q] and j <= LAST[q] for q in before)
                    ]

                    @pl.when(any_of(me, new))
                    def _():
                        pl.semaphore_wait(ready_kv.at[j], 1)

                @pl.when(me != j)
                def _():
                    returned(r, head, j).start()

                @pl.when(me == j)
                def _():
                    a_buf[r, head] = o_stage[r, j]

    for r in RANK_ORDER:

        @pl.when(any_of(me, PLACE[r]))
        def _():
            attend(r)

    half = ROWS // 2
    lower, upper = pl.ds(0, half), pl.ds(half, half)

    def hop(r, block, rows, to, n):
        ref = x_buf.at[r, block] if rows is None else x_buf.at[r, block, rows]
        return pltpu.make_async_remote_copy(
            src_ref=ref,
            dst_ref=ref,
            send_sem=g_send.at[r],
            recv_sem=g_recv.at[r, RELAY_SEM[n]],
            device_id={"tp": to},
            device_id_type=MESH,
        )

    def sent(r, n):
        return hop(r, *(
            (tp, lower, right, 0),
            (tp, upper, right, 1),
            (tp, upper, left, 2),
            (tp, lower, left, 3),
            (left, lower, right, 4),
            (right, upper, left, 5),
            (tp, None, partner, 6),
            (left, None, partner, 7),
            (right, None, partner, 8),
            (far, None, partner, 9),
        )[n])

    def other(t):
        return t + 1 - 2 * lax.rem(t, 2)

    def received(r, n):
        return hop(r, *(
            (left, lower, left, 0),
            (left, upper, left, 1),
            (right, upper, right, 2),
            (right, lower, right, 3),
            (far, lower, left, 4),
            (far, upper, right, 5),
            (other(tp), None, partner, 6),
            (other(left), None, partner, 7),
            (other(right), None, partner, 8),
            (other(far), None, partner, 9),
        )[n])

    rows_each = ROWS // n_tp
    width = wo.shape[1]

    def column_copy(r, to):
        return pltpu.make_async_remote_copy(
            src_ref=y_buf.at[r, pl.ds(pl.multiple_of(to * rows_each, rows_each), rows_each)],
            dst_ref=o_buf.at[r, :, pl.ds(pl.multiple_of(tp * width, width), width)],
            send_sem=y_send.at[r],
            recv_sem=y_recv.at[r],
            device_id={"tp": to},
            device_id_type=MESH,
        )

    def columns_all(r):
        rest = pl.ds(0, (n_tp - 1) * rows_each)
        return pltpu.make_async_remote_copy(
            src_ref=y_buf.at[r, rest],
            dst_ref=y_buf.at[r, rest],
            send_sem=y_send.at[r],
            recv_sem=y_recv.at[r],
            device_id={"tp": partner},
            device_id_type=MESH,
        )

    loads[8].wait()
    for t in range(n_tp):

        @pl.when(tp > t)
        def _():
            pl.semaphore_wait(ready_tp.at[t], 1)


    def handed_back(r, count):
        return pltpu.make_async_remote_copy(
            src_ref=o_stage.at[r, pl.ds(0, count)],
            dst_ref=a_buf.at[r, pl.ds(0, count)],
            send_sem=o_send.at[r],
            recv_sem=o_recv.at[r],
            device_id={"kv": jnp.int32(0)},
            device_id_type=MESH,
        )

    def own(r):
        inside = any_of(me, PLACE[r])

        @pl.when(inside)
        def _():
            handed_back(r, n_head - 1).wait_recv()

        @pl.when(jnp.logical_not(inside))
        def _():
            handed_back(r, n_head).wait_recv()

        x_buf[r, tp] = a_buf[r].reshape(n_head * HD, ROWS).T
        for n in (0, 2, 1, 3, 6):
            sent(r, n).start()

    def relay(r):
        received(r, 0).wait_recv()
        sent(r, 4).start()
        received(r, 2).wait_recv()
        sent(r, 5).start()
        received(r, 1).wait_recv()
        sent(r, 7).start()
        received(r, 3).wait_recv()
        sent(r, 8).start()

    def across(r):
        hop(r, far, None, left, 4).wait_recv()
        sent(r, 9).start()

    def mix(r):
        blocks = x_buf.at[r, pl.ds(0, n_tp // 2)]
        pltpu.make_async_remote_copy(
            src_ref=blocks,
            dst_ref=blocks,
            send_sem=g_send.at[r],
            recv_sem=g_recv.at[r, RELAY_SEM[6]],
            device_id={"tp": partner},
            device_id_type=MESH,
        ).wait_recv()
        rows = jnp.concatenate([x_buf[r, g] for g in range(n_tp)], axis=1)
        y_buf[r] = nn(rows, wo[...]).astype(BF)
        for step in range(1, n_tp):
            column_copy(r, lax.rem(tp + step, n_tp)).start()
        mine = pl.ds(pl.multiple_of(tp * rows_each, rows_each), rows_each)
        o_buf[r, :, pl.ds(pl.multiple_of(tp * width, width), width)] = y_buf[r, mine]

    def stage(step, r):
        @pl.when(me <= LAST[r])
        def _():
            step(r)

    first, second, third, last = RANK_ORDER
    for step, r in (
        (own, first), (own, second), (relay, first), (own, third), (relay, second), (own, last),
        (across, first), (relay, third), (across, second), (mix, first), (relay, last),
        (across, third), (mix, second), (across, last), (mix, third), (mix, last),
    ):
        stage(step, r)

    for r in range(n_seq):

        @pl.when(me > LAST[r])
        def _():
            o_buf[r] = jnp.zeros(o_buf.shape[1:], BF)

    for r in range(n_seq):

        @pl.when(me <= LAST[r])
        def _():
            columns_all(r).wait_recv()

    many = rows_each * n_seq
    want = iota((many, many), 0)
    have = iota((many, many), 1)
    pick = jnp.zeros((many, many), F32)
    for r in range(n_seq):
        hit = (have == r * rows_each + want // n_seq) & (lax.rem(want, n_seq) == seq_of[r])
        pick = jnp.where(hit, 1.0, pick)
    pick = pick.astype(BF)
    for c in range(n_tp):
        cols = slice(c * width, (c + 1) * width)
        rows = o_buf[:, :, cols].reshape(many, width)
        out_ref[:, :, cols] = nn(pick, rows).astype(BF).reshape(rows_each, n_seq, width)

    for r in range(n_seq):
        inside = any_of(me, PLACE[r])

        @pl.when((me <= LAST[r]) & inside)
        def _():
            departures(r, n_head - 1).wait_send()

        @pl.when((me <= LAST[r]) & jnp.logical_not(inside))
        def _():
            departures(r, n_head).wait_send()

        def returned_all(count):
            return pltpu.make_async_remote_copy(
                src_ref=o_stage.at[r, pl.ds(0, count)],
                dst_ref=o_stage.at[r, pl.ds(0, count)],
                send_sem=o_send.at[r],
                recv_sem=o_recv.at[r],
                device_id={"kv": jnp.int32(0)},
                device_id_type=MESH,
            )

        @pl.when(inside & (me <= LAST[r]))
        def _():
            returned_all(LAST[r]).wait_send()

        if any(p > LAST[r] for p in PLACE[r]):

            @pl.when(inside & (me > LAST[r]))
            def _():
                returned_all(LAST[r] + 1).wait_send()

        @pl.when(me <= LAST[r])
        def _():
            blocks = x_buf.at[r, pl.ds(0, 2 + 1 + n_tp // 2)]
            pltpu.make_async_remote_copy(
                src_ref=blocks,
                dst_ref=blocks,
                send_sem=g_send.at[r],
                recv_sem=g_recv.at[r, 0],
                device_id={"tp": partner},
                device_id_type=MESH,
            ).wait_send()
            columns_all(r).wait_send()


def body(tokens, lengths, chosen, w_query, w_key, w_value, w_gate, pool_weights, w_out):
    rows, n_seq, depth = tokens.shape
    n_head = w_query.shape[1] // HD
    n_kv, n_tp = lax.axis_size("kv"), lax.axis_size("tp")
    gate_rows = jnp.transpose(w_gate, (1, 2, 0))
    width = w_out.shape[1]
    total = rows * n_seq
    vmem = pl.BlockSpec(memory_space=pltpu.VMEM)
    hbm = pl.BlockSpec(memory_space=pl.ANY)
    dma = pltpu.SemaphoreType.DMA
    full = n_kv * rows

    def whole(*refs):
        kernel(n_kv, n_tp, n_seq, n_head, *refs)

    return pl.pallas_call(
        whole,
        out_shape=jax.ShapeDtypeStruct((rows // n_tp, n_seq, n_tp * width), BF),
        in_specs=[hbm] * 9,
        out_specs=vmem,
        scratch_shapes=[
            pltpu.VMEM((rows, n_seq, depth), BF),
            pltpu.VMEM((total, depth), BF),
            pltpu.VMEM((3, depth, n_head * HD), BF),
            pltpu.VMEM(gate_rows.shape, BF),
            pltpu.VMEM(pool_weights.shape, F32),
            pltpu.VMEM(w_out.shape, BF),
            pltpu.SMEM(lengths.shape, jnp.int32),
            pltpu.SMEM(chosen.shape, jnp.int32),
            pltpu.VMEM((total, total), BF),
            pltpu.VMEM((n_seq * n_head, MSG, rows), BF),
            pltpu.VMEM((n_seq, n_kv, MSG, rows), BF),
            pltpu.VMEM((128, full), BF),
            pltpu.VMEM((128, full), BF),
            pltpu.VMEM((128, full), BF),
            pltpu.VMEM((2 * HD, rows), F32),
            pltpu.VMEM((2 * HD, rows), F32),
            pltpu.VMEM((n_seq, n_kv, HD, rows), BF),
            pltpu.VMEM((n_seq, n_head, HD, rows), BF),
            pltpu.VMEM((n_seq, n_tp, rows, n_head * HD), BF),
            pltpu.VMEM((n_seq, rows, width), BF),
            pltpu.VMEM((n_seq, rows // n_tp, n_tp * width), BF),
            dma((9,)),
            dma((n_seq,)),
            dma((FIRST[-1] + LAST[-1] + 1,)),
            dma((n_seq,)),
            dma((n_seq,)),
            dma((n_seq,)),
            dma((n_seq, 6)),
            dma((n_seq,)),
            dma((n_seq,)),
            pltpu.SemaphoreType.REGULAR((n_kv,)),
            pltpu.SemaphoreType.REGULAR((n_tp,)),
        ],
        compiler_params=pltpu.CompilerParams(
            collective_id=0, has_side_effects=True, vmem_limit_bytes=60 * 2**20
        ),
    )(tokens, lengths, chosen, w_query, w_key, w_value, gate_rows, pool_weights, w_out)


def solution(mesh):
    placed = (
        P("kv", "grp", None),
        P("grp"),
        P("grp", "tp", "kv", None),
        P(None, "tp"),
        P(None, "tp"),
        P(None, "tp"),
        P(None, None, "tp"),
        P(),
        P(None, "tp"),
    )
    return jax.shard_map(
        body, mesh=mesh, in_specs=placed, out_specs=P(("kv", "tp"), "grp", None), check_vma=False
    )
```
